128 devices in a mesh: tp: 16 (over z, y), dp: 8 (over x, core).
Axes of the slice: x: 4, y: 4, z: 4, core: 2. Of those that a mesh axis runs over, the one named last changes fastest.
Arguments:
- activation_rows: bfloat16 [2048, 4096], P(None, 'dp'), may hold values from -24 to 24
- fresh_spans: int32 [256], P('dp'), may hold values from 1 to 8, 768 in all
- entry_rescale_vector: float32 [2, 4096], P(None, 'dp'), may hold values from 0.1 to 1.9
- probe_kernel: bfloat16 [2, 4096, 4096], P(None, 'dp', 'tp'), may hold values from -0.09375 to 0.09375
- retention_kernel: bfloat16 [2, 4096, 4096], P(None, 'dp', 'tp'), may hold values from -0.09375 to 0.09375
- content_kernel: bfloat16 [2, 4096, 4096], P(None, 'dp', 'tp'), may hold values from -0.09375 to 0.09375
- valve_kernel: bfloat16 [2, 4096, 4096], P(None, 'dp', 'tp'), may hold values from -0.09375 to 0.09375
- retention_minimum: float32 [2, 4096], P(None, 'tp'), may hold values from 0 to 0.99
- extra_attenuation: float32 [2, 2048, 32], P(None, 'dp', 'tp'), may hold values from -0.7 to 0
- channel_rescale_vector: float32 [2, 4096], P(None, 'tp'), may hold values from 0.1 to 1.9
- emission_kernel: bfloat16 [2, 4096, 4096], P(None, 'tp', 'dp'), may hold values from -0.09375 to 0.09375
- memory_grids: float32 [2, 256, 32, 128, 128], P(None, 'dp', 'tp'), may hold values from -0.6 to 0.6
Outputs:
- mixed: bfloat16 [2048, 4096], P(None, 'dp')
- new_states: float32 [2, 256, 32, 128, 128], P(None, 'dp', 'tp')
The draws below stay inside these ranges and needn't reach their ends.
Inputs may be any that keep to these rules, and one draw needn't show every extreme that they name: `fresh_spans`: each sequence has at least one live slot.
All inputs are finite; a program needn't handle non-finite values. No bound on the sum of `fresh_spans` on one device may be relied on, other than what follows from the above.
Results may differ from the reference program's by a relative error of at most 0.017.
Values may be sent and summed in bfloat16 or wider, within the bound.
No kernel may reach another device: no remote copies, remote signals or barrier semaphores. Data moves between devices by JAX's collectives and lax.ppermute only.
A program may use at most 128 MiB of HBM per device.

```python
import math
import jax
import jax.numpy as jnp
import numpy as np
from jax import lax

D = 4096
HEADS = 32
DK = 128
DV = 128
NEW = 8
BLOCKS = 2
SEQS = 256
ROWS = 2048
HK = 4096
HV = 4096
N_DP = 8


def draw_activation_rows(key, part):
    column_scale = jnp.exp(jnp.linspace(0.0, math.log(4.0), D, dtype=jnp.float32))[None, :]
    base = jnp.clip(jax.random.normal(key, (ROWS, D), jnp.float32), -6.0, 6.0)
    return jnp.clip(base * column_scale, -24.0, 24.0).astype(jnp.bfloat16)


def draw_extra_attenuation(key, part):
    hits = jax.random.randint(jax.random.fold_in(key, 3), (BLOCKS, ROWS, HEADS), 0, 10) == 0
    depth = jax.random.uniform(jax.random.fold_in(key, 4), (BLOCKS, ROWS, HEADS), jnp.float32, math.log(0.5), math.log(0.8))
    return jnp.where(hits, depth, jnp.zeros_like(depth)).astype(jnp.float32)


def levels(stream_key, dims, cuts, smallest, high):
    factor_of = 1.0
    for position, parts in cuts:
        heights = jax.random.uniform(jax.random.fold_in(jax.random.fold_in(stream_key, 6), position), (parts,), jnp.float32, smallest / len(cuts), high / len(cuts))
        factor_of = factor_of * jnp.repeat(jnp.exp(heights), dims[position] // parts).reshape((-1,) + (1,) * (len(dims) - 1 - position))
    return factor_of


def length_profile(count, total, most, skew):
    loads = [(1 << 20) // math.isqrt(standing ** skew) + 1 for standing in range(2, count + 1)]
    surplus, holding = total - most - (count - 1), [1] * (count - 1)
    while surplus > 0:
        candidates = [i for i in range(count - 1) if holding[i] < most]
        mass, left = sum([loads[i] for i in candidates]), surplus
        for i in candidates:
            more = min(most - holding[i], max(1, left * loads[i] // mass), surplus)
            holding[i] = holding[i] + more
            surplus = surplus - more
    return np.array([most] + holding)


def ragged(stream_key, count, total, reach, skew):
    if count == 2:
        one = jax.random.randint(stream_key, (), max(1, total - reach), min(reach, total - 1) + 1)
        return jnp.stack([one, total - one])
    tallies = jnp.asarray(length_profile(count, total, reach, skew), jnp.int32)
    twos = (count - 1) // 2
    giver, receiver = tallies[1:1 + 2 * twos:2], tallies[2:2 + 2 * twos:2]
    room = jnp.minimum(giver - 1, reach - receiver)
    passed = jax.random.randint(jax.random.fold_in(stream_key, 1), (twos,), 0, 1 << 20) % (room + 1)
    tallies = tallies.at[1:1 + 2 * twos:2].set(giver - passed).at[2:2 + 2 * twos:2].set(receiver + passed)
    return tallies[jax.random.permutation(jax.random.fold_in(stream_key, 2), count)]


def noise(rng, dims, scale, most, split=(), kind=jnp.bfloat16):
    result = jax.random.normal(rng, dims, jnp.float32) * scale
    if len(split) > 0:
        result = levels(rng, dims, split, -0.22, 0.18) * result
    return jnp.clip(result, min=-most, max=most).astype(kind)


def setup_inputs(seed: int = 0) -> dict:
    splits = jax.random.split(jax.random.key(seed), 13)
    return {
        "activation_rows": draw_activation_rows(jax.random.fold_in(splits[12], 71), 0),
        "fresh_spans": ragged(splits[1], SEQS, 3 * SEQS, NEW, 2).astype(jnp.int32),
        "entry_rescale_vector": jnp.clip(1.0 + 0.18 * jax.random.normal(splits[2], (BLOCKS, D), jnp.float32), 0.1, 1.9),
        "probe_kernel": noise(splits[3], (BLOCKS, D, HK), D ** -0.5, 0.09375, ((1, 8), (2, 16))),
        "retention_kernel": noise(splits[4], (BLOCKS, D, HK), D ** -0.5, 0.09375, ((1, 8), (2, 16))),
        "content_kernel": noise(splits[5], (BLOCKS, D, HV), D ** -0.5, 0.09375, ((1, 8), (2, 16))),
        "valve_kernel": noise(splits[6], (BLOCKS, D, HV), D ** -0.5, 0.09375, ((1, 8), (2, 16))),
        "retention_minimum": jnp.clip(0.99 * jax.random.uniform(splits[7], (BLOCKS, HK), jnp.float32) ** levels(splits[7], (BLOCKS, HK), ((1, 16),), -0.2, 0.2), 0.0, 0.99),
        "extra_attenuation": draw_extra_attenuation(jax.random.fold_in(splits[12], 71), 0),
        "channel_rescale_vector": jnp.clip(1.0 + 0.18 * jax.random.normal(splits[9], (BLOCKS, HV), jnp.float32), 0.1, 1.9),
        "emission_kernel": noise(splits[10], (BLOCKS, HV, D), HV ** -0.5, 0.09375, ((1, 16), (2, 8))),
        "memory_grids": noise(splits[11], (BLOCKS, SEQS, HEADS, DK, DV), 0.1, 0.6, ((1, 8), (2, 16)), jnp.float32),
    }


EPSILON = 1e-05

def update_tick(probe_scores, retention_scores, content_scores, valve_scores, minimum_bound, spike_ledger, attention_multiplier, stream_spans, memory_grid):
    stream_tally = memory_grid.shape[0]
    attention_tally = memory_grid.shape[1]
    key_dim = memory_grid.shape[2]
    value_dim = memory_grid.shape[3]
    position_tally = probe_scores.shape[0] // stream_tally

    def split_heads(array, width):
        return array.astype(jnp.float32).reshape(stream_tally, position_tally, attention_tally, width)
    queries = jax.nn.silu(split_heads(probe_scores, key_dim))
    forget_in = split_heads(retention_scores, key_dim)
    lower_heads = minimum_bound.reshape(attention_tally, key_dim)
    retention_sigmoid = lower_heads + (1.0 - lower_heads) * jax.nn.sigmoid(forget_in)
    key_vecs = (1.0 - lower_heads) * jax.nn.sigmoid(-forget_in)
    log_attenuation = jnp.log(retention_sigmoid) + spike_ledger.reshape(stream_tally, position_tally, attention_tally)[..., None]
    values = split_heads(content_scores, value_dim)
    positions = lax.broadcasted_iota(jnp.int32, (stream_tally, position_tally), 1)
    live_mask = positions < stream_spans[:, None].astype(jnp.int32)

    def advance(matrix, inputs):
        query_now, key_now, decay_now, value_now, live_now = inputs
        updated = jnp.exp(decay_now)[..., None] * matrix + key_now[..., None] * value_now[..., None, :]
        matrix = jnp.where(live_now[:, None, None, None], updated, matrix)
        readout = jnp.einsum('shkv,shk->shv', matrix, query_now, precision=lax.Precision.HIGHEST)
        return (matrix, readout)
    ending_emission, readouts = lax.scan(advance, memory_grid, (jnp.moveaxis(queries, 1, 0), jnp.moveaxis(key_vecs, 1, 0), jnp.moveaxis(log_attenuation, 1, 0), jnp.moveaxis(values, 1, 0), jnp.moveaxis(live_mask, 1, 0)))
    readouts = jnp.moveaxis(readouts, 0, 1)
    normed = readouts * lax.rsqrt(lax.optimization_barrier(jnp.mean(readouts * readouts, axis=-1, keepdims=True)) + EPSILON)
    normed = normed * attention_multiplier.reshape(attention_tally, value_dim) * jax.nn.silu(split_heads(valve_scores, value_dim))
    normed = normed * live_mask.astype(jnp.float32)[..., None, None]
    return (normed.reshape(stream_tally * position_tally, attention_tally * value_dim).astype(jnp.bfloat16), ending_emission)

def blocked_product(normed, weight):
    width = D // N_DP
    total = jnp.zeros((normed.shape[0], weight.shape[1]), jnp.float32)
    for index in range(N_DP):
        partial_value = jnp.dot(normed[:, index * width:(index + 1) * width], weight[index * width:(index + 1) * width], preferred_element_type=jnp.float32)
        rounded = lax.optimization_barrier(partial_value.astype(jnp.bfloat16))
        total = total + rounded.astype(jnp.float32)
    return total

def reference(activation_rows, fresh_spans, entry_rescale_vector, probe_kernel, retention_kernel, content_kernel, valve_kernel, retention_minimum, extra_attenuation, channel_rescale_vector, emission_kernel, memory_grids):
    residual = activation_rows
    finals = []
    for layer_index in range(BLOCKS):
        current = residual.astype(jnp.float32)
        row_scale = lax.rsqrt(lax.optimization_barrier(jnp.mean(current * current, axis=1)) + EPSILON)
        normed = (current * entry_rescale_vector[layer_index]).astype(jnp.bfloat16)
        mapped_activation = [(blocked_product(normed, weight[layer_index]) * row_scale[:, None]).astype(jnp.bfloat16) for weight in (probe_kernel, retention_kernel, content_kernel, valve_kernel)]
        attention_yields, ending_emission = update_tick(mapped_activation[0], mapped_activation[1], mapped_activation[2], mapped_activation[3], retention_minimum[layer_index], extra_attenuation[layer_index], channel_rescale_vector[layer_index], fresh_spans, memory_grids[layer_index])
        finals.append(ending_emission)
        update = jnp.dot(attention_yields, emission_kernel[layer_index], preferred_element_type=jnp.float32).astype(jnp.bfloat16)
        residual = (current + update.astype(jnp.float32)).astype(jnp.bfloat16)
    return (residual, jnp.stack(finals))
```

```python
import functools

import jax
import jax.numpy as jnp
from jax import lax
from jax.experimental import pallas as pl
from jax.experimental.pallas import tpu as pltpu
from jax.sharding import PartitionSpec as P

D = 4096
BLOCKS = 2
EPSILON = 1e-05
GROUPS = 8
CAP = 128
LIVE = 768
SLOTS = 8
TINY = 1.2e-38
F32 = jnp.float32
BF16 = jnp.bfloat16
VM = pl.BlockSpec(memory_space=pltpu.VMEM)


def iota(shape, dim):
    return lax.broadcasted_iota(jnp.int32, shape, dim)


def mm(a, b, dims=((1,), (0,)), **kw):
    return lax.dot_general(a, b, (dims, ((), ())), preferred_element_type=F32, **kw)


def call(body, out_shape, in_specs, out_specs, name, flops=0, moved=0, vmem=16, **kw):
    return pl.pallas_call(
        body,
        out_shape=out_shape,
        in_specs=in_specs,
        out_specs=out_specs,
        name=name,
        cost_estimate=pl.CostEstimate(flops=flops, bytes_accessed=moved, transcendentals=0),
        compiler_params=pltpu.CompilerParams(vmem_limit_bytes=vmem << 20),
        **kw,
    )


def place_of():
    tp, dp = lax.axis_index("tp"), lax.axis_index("dp")
    return dp % 2, dp // 2, tp % 4


def index_body(spans_ref, pos_ref, caprow_ref, capcol_ref):
    spans = spans_ref[...]
    seqs = spans.shape[1]
    rows = seqs * SLOTS
    before = (iota((seqs, seqs), 0) < iota((seqs, seqs), 1)).astype(F32)
    spread = (iota((seqs, rows), 0) == iota((seqs, rows), 1) // SLOTS).astype(F32)
    start = mm(mm(spans, before), spread)
    span = mm(spans, spread)
    slot = (iota((GROUPS, rows), 1) % SLOTS).astype(F32)
    pos_ref[...] = jnp.where(slot < span, start + slot, -1.0)
    count_col = jnp.sum(spans, axis=1, keepdims=True)
    upto = (iota((GROUPS, GROUPS), 1) <= iota((GROUPS, GROUPS), 0)).astype(F32)
    count_row = mm(jnp.ones((GROUPS, seqs), F32), spans, ((1,), (1,)))
    end_col = mm(upto, jnp.broadcast_to(count_col, (GROUPS, 128)))[:, :1]
    end_row = mm(count_row, upto, ((1,), (1,)))[:1]
    g = iota((GROUPS, LIVE), 1).astype(F32)
    caprow_ref[...] = g[:1] + jnp.sum(
        jnp.where(g >= end_col, CAP - count_col, 0.0), axis=0, keepdims=True
    )
    g = iota((LIVE, GROUPS), 0).astype(F32)
    cap = g[:, :1] + jnp.sum(
        jnp.where(g >= end_row, CAP - count_row[:1], 0.0), axis=1, keepdims=True
    )
    capcol_ref[...] = jnp.broadcast_to(cap, (LIVE, 128))


def index_maps(spans):
    rows = spans.shape[1] * SLOTS
    return call(
        index_body,
        (
            jax.ShapeDtypeStruct((GROUPS, rows), F32),
            jax.ShapeDtypeStruct((1, LIVE), F32),
            jax.ShapeDtypeStruct((LIVE, 128), F32),
        ),
        [VM],
        (VM, VM, VM),
        "index_maps",
        1 << 20,
        1 << 20,
        4,
    )(spans)


def chosen(pos_row, cap=CAP):
    shape = (cap, pos_row.shape[1])
    return (iota(shape, 0).astype(F32) == pos_row).astype(BF16)


def project(x, layer, gain_ref, weights, out_ref, at):
    normed = (x * gain_ref[layer : layer + 1, :]).astype(BF16)
    width = weights[0].shape[2]
    for n, weight in enumerate(weights):
        out_ref[at, :CAP, n * width : (n + 1) * width] = mm(normed, weight[layer]).astype(BF16)
    squares = x * x
    squares = sum(squares[:, n : n + CAP] for n in range(0, x.shape[1], CAP))
    ones = jnp.ones((8, CAP), BF16)
    high = squares.astype(BF16)
    low = (squares - high.astype(F32)).astype(BF16)
    squares = mm(ones, high, ((1,), (1,))) + mm(ones, low, ((1,), (1,)))
    high = squares.astype(BF16)
    low = (squares - high.astype(F32)).astype(BF16)
    out_ref[at, CAP:, :] = jnp.zeros((8, out_ref.shape[2]), BF16)
    out_ref[at, CAP:, :CAP] = high
    out_ref[at, CAP:, CAP : 2 * CAP] = low


def first_body(layer, x_ref, pos_ref, gain_ref, *refs):
    weights, (own_ref, sent_ref, x_out) = refs[:4], refs[4:]
    core, _, _ = place_of()

    def step(i, _):
        for side, out_ref in ((1, sent_ref), (0, own_ref)):
            j = 2 * i + (1 - core if side else core)
            x = mm(chosen(pos_ref[pl.ds(j, 1), :]), x_ref[j])
            x_out[j] = x.astype(BF16)
            project(x, layer, gain_ref, weights, out_ref, i)
        return 0

    lax.fori_loop(0, 4, step, 0)


def gathered(y, updates, update):
    part = updates[0].shape[0]
    for d, u in enumerate(updates):
        update[pl.ds(pl.multiple_of(((y + 4 - d) % 4) * part, part), part), :] = u[...]


def next_body(layer, x_ref, caprow_ref, u0, u1, u2, u3, gain_ref, *refs):
    weights, (own_ref, sent_ref, x_out, update) = refs[:4], refs[4:]
    core, _, y = place_of()
    gathered(y, (u0, u1, u2, u3), update)

    def step(i, _):
        for side, out_ref in ((1, sent_ref), (0, own_ref)):
            j = 2 * i + (1 - core if side else core)
            picked = chosen(caprow_ref[...] - (j * CAP).astype(F32))
            x = (x_ref[j].astype(F32) + mm(picked, update[...])).astype(BF16)
            x_out[j] = x
            project(x.astype(F32), layer, gain_ref, weights, out_ref, i)
        return 0

    lax.fori_loop(0, 4, step, 0)


def projections(layer, x, maps, updates, gain, weights):
    features = x.shape[-1]
    width = 4 * weights[0].shape[2]
    args = [x, maps, *updates, gain, *weights]
    return call(
        functools.partial(next_body if updates else first_body, layer),
        (
            jax.ShapeDtypeStruct((4, CAP + 8, width), BF16),
            jax.ShapeDtypeStruct((4, CAP + 8, width), BF16),
            jax.ShapeDtypeStruct((GROUPS, CAP, features), BF16),
        ),
        [VM] * len(args),
        (VM,) * 3,
        "next_projection" if updates else "first_projection",
        2 << 30,
        6 << 20,
        scratch_shapes=[pltpu.VMEM((LIVE, features), BF16)] if updates else [],
    )(*args)


def pair_body(own_ref, got_ref, keep_ref, *sent):
    _, x, _ = place_of()

    def step(d, keep):
        at = (x + d) % 4
        squares = own_ref[at, CAP:, : 2 * CAP].astype(F32) + got_ref[at, CAP:, : 2 * CAP].astype(F32)
        squares = squares[:, :CAP] + squares[:, CAP:]
        high = squares if keep else squares.astype(BF16)
        low = squares - high.astype(F32)
        out = keep_ref if keep else sent[d - 1]
        kind = out.dtype
        out[CAP:, :CAP] = high.astype(kind)
        out[CAP:, CAP : 2 * CAP] = low.astype(kind)
        for n in range(0, own_ref.shape[2], 256):
            piece = own_ref[at, :CAP, n : n + 256].astype(F32) + got_ref[at, :CAP, n : n + 256].astype(F32)
            out[:CAP, n : n + 256] = piece.astype(kind)
        out[CAP:, 2 * CAP :] = jnp.zeros((8, own_ref.shape[2] - 2 * CAP), kind)

    for d in (2, 1, 3, 0):
        step(d, d == 0)


def pair_sum(own, got):
    rows, width = own.shape[1:]
    return call(
        pair_body,
        (jax.ShapeDtypeStruct((rows, width), F32),)
        + (jax.ShapeDtypeStruct((rows, width), BF16),) * 3,
        [VM, VM],
        (VM,) * 4,
        "pair_sum",
        1 << 20,
        4 << 20,
        8,
    )(own, got)


def roll_slots(x, d):
    return pltpu.roll(x, d, 1) if d else x


def read_body(layer, keep, r1, r2, r3, pos_ref, low_ref, extra_ref, chan_ref, states, *refs):
    out_rows, kk, vv, held, wide, alive, qa, reads, gates, sems = refs
    heads = kk.shape[0]
    seqs = kk.shape[1]
    rows = seqs * SLOTS
    dim = 128
    parts = sems.shape[0]
    each = seqs // parts

    def fetch(n):
        return pltpu.make_async_copy(
            states.at[layer, pl.ds(n * each, each)], held.at[pl.ds(n * each, each)], sems.at[n]
        )

    for n in range(parts):
        fetch(n).start()
    total = keep[...] + r1[...].astype(F32) + r2[...].astype(F32) + r3[...].astype(F32)
    squares = total[CAP : CAP + 1, :CAP] + total[CAP : CAP + 1, CAP : 2 * CAP]
    scale = lax.rsqrt(squares / D + EPSILON)
    eye = iota((CAP, CAP), 0) == iota((CAP, CAP), 1)
    scale = jnp.sum(jnp.where(eye, scale, 0.0), axis=1, keepdims=True)
    scaled = (total[:CAP] * scale).astype(BF16)
    picked = chosen(pos_ref[pl.ds(lax.axis_index("dp"), 1), :])
    wide[...] = mm(picked, scaled, ((0,), (0,)))
    alive[...] = mm(picked, jnp.ones((CAP, dim), BF16), ((0,), (0,)))
    some = 8
    chunk = some * SLOTS
    shape = (some, SLOTS, dim)

    def prepare(n, _):
        h, c = n // (seqs // some), n % (seqs // some)
        at = pl.ds(pl.multiple_of(c * chunk, chunk), chunk)
        here = pl.ds(c * some, some)

        def part(k):
            lanes = pl.ds(pl.multiple_of((k * heads + h) * dim, dim), dim)
            return wide[at, lanes].reshape(shape)

        lanes = pl.ds(pl.multiple_of(h * dim, dim), dim)
        low = low_ref[layer : layer + 1, lanes]
        chan = chan_ref[layer : layer + 1, lanes]
        both = extra_ref[layer, at, :]
        extra = jnp.sum(jnp.where(iota(both.shape, 1) == h, both, 0.0), axis=1, keepdims=True)
        live = alive[at, :].reshape(shape) > 0.5
        slot = iota(shape, 1)
        query = jax.nn.silu(part(0))
        forget = part(1)
        left = low + (1.0 - low) * jax.nn.sigmoid(forget)
        key = jnp.where(live, (1.0 - low) * jax.nn.sigmoid(-forget), 0.0)
        value = part(2)
        decay = jnp.log(jnp.maximum(left, TINY)) + jnp.broadcast_to(extra, (chunk, dim)).reshape(shape)
        decay = jnp.where(live, decay, 0.0)
        for d in (1, 2, 4):
            decay = decay + jnp.where(slot >= d, roll_slots(decay, d), 0.0)
        ones = jnp.ones((dim, dim), BF16)
        read = jnp.zeros(shape, F32)
        for d in range(SLOTS):
            term = query * roll_slots(key, d)
            if d:
                fade = jnp.exp(jnp.minimum(decay - roll_slots(decay, d), 0.0))
                term = jnp.where(slot >= d, term * fade, 0.0)
            weight = mm(term.astype(BF16).reshape(chunk, dim), ones)
            read = read + weight.reshape(shape) * roll_slots(value, d)
        reads[h, here] = read
        qa[h, here] = (query * jnp.exp(decay)).astype(BF16)
        last = decay[:, SLOTS - 1 :, :]
        whole = jnp.exp(last)
        high = whole.astype(BF16).astype(F32)
        tail = jnp.where(slot == 0, high, jnp.where(slot == 1, whole - high, 0.0))
        kk[h, here, :SLOTS, :] = (key * jnp.exp(last - decay)).astype(BF16)
        kk[h, here, SLOTS:, :] = tail.astype(BF16)
        vv[h, here] = value.astype(BF16)
        gates[h, here] = jax.nn.silu(part(3)) * chan
        return 0

    lax.fori_loop(0, heads * (seqs // some), prepare, 0)

    def apply(n, _):
        fetch(n).wait()
        for s in range(each):
            at = n * each + s
            for h in range(heads):
                reads[h, at] += mm(qa[h, at], held[at, h].astype(BF16))
        return 0

    lax.fori_loop(0, parts, apply, 0)
    for h in range(heads):
        read = reads[h]
        mean = jnp.mean(read * read, axis=-1, keepdims=True)
        head = (read * lax.rsqrt(mean + EPSILON) * gates[h]).astype(BF16).reshape(rows, dim)
        out_rows[:, h * dim : (h + 1) * dim] = mm(picked, head).astype(BF16)


def read_states(layer, keep, got, pos, low, extra, chan, states):
    _, seqs, heads, dim, _ = states.shape
    return call(
        functools.partial(read_body, layer),
        (
            jax.ShapeDtypeStruct((CAP, heads * dim), BF16),
            jax.ShapeDtypeStruct((heads, seqs, 2 * SLOTS, dim), BF16),
            jax.ShapeDtypeStruct((heads, seqs, SLOTS, dim), BF16),
        ),
        [VM] * 8 + [pl.BlockSpec(memory_space=pl.ANY)],
        (VM,) * 3,
        "read_states",
        1 << 30,
        6 << 20,
        20,
        scratch_shapes=[
            pltpu.VMEM((seqs, heads, dim, dim), F32),
            pltpu.VMEM((seqs * SLOTS, 4 * heads * dim), F32),
            pltpu.VMEM((seqs * SLOTS, dim), F32),
            pltpu.VMEM((heads, seqs, SLOTS, dim), BF16),
            pltpu.VMEM((heads, seqs, SLOTS, dim), F32),
            pltpu.VMEM((heads, seqs, SLOTS, dim), F32),
            pltpu.SemaphoreType.DMA((8,)),
        ],
    )(keep, *got, pos, low, extra, chan, states)


def write_body(kk, vv, state_ref, *refs):
    out_state = refs[-1]
    dim = 128
    zero = jnp.zeros((SLOTS, dim), BF16)
    ones = jnp.ones((SLOTS, dim), BF16)

    def one(s, _):
        for h in range(state_ref.shape[2]):
            state = state_ref[0, s, h]
            values = jnp.concatenate(
                [jnp.concatenate([vv[h, s], zero], 1), jnp.concatenate([zero, ones], 1)], 0
            )
            both = mm(kk[h, s], values, ((0,), (0,)))
            out_state[0, s, h] = both[:, dim:] * state + both[:, :dim]
        return 0

    lax.fori_loop(0, state_ref.shape[1], one, 0)


def write_states(layer, kk, vv, states, written):
    _, seqs, heads, dim, _ = states.shape
    here = 4
    block = pl.BlockSpec((1, here, heads, dim, dim), lambda i: (layer, i, 0, 0, 0))
    small = lambda a: pl.BlockSpec((heads, here, a.shape[2], dim), lambda i: (0, i, 0, 0))
    more = [] if written is None else [written]
    return call(
        write_body,
        jax.ShapeDtypeStruct(states.shape, F32),
        [small(kk), small(vv), block] + [pl.BlockSpec(memory_space=pl.ANY)] * len(more),
        block,
        "write_states",
        10 << 30,
        8 << 20,
        8,
        grid=(seqs // here,),
        input_output_aliases={3: 0} if more else {},
    )(kk, vv, states, *more)


def emit_body(layer, *refs):
    blocks, (cap_ref, weight, keep_ref, s1, s2, s3, held) = refs[:8], refs[8:]
    core, x, y = place_of()
    for side in range(2):
        for d in range(4):
            j = 2 * ((x + 4 - d) % 4) + (1 - core if side else core)
            held[pl.ds(pl.multiple_of(j * CAP, CAP), CAP), :] = blocks[4 * side + d][...]
    part = keep_ref.shape[0]
    lanes = iota((part, GROUPS * CAP), 1).astype(F32)
    for d in (2, 1, 3, 0):
        at = pl.multiple_of(((y + d) % 4) * part, part)
        picked = (cap_ref[pl.ds(at, part), :1] == lanes).astype(BF16)
        rows = mm(picked, held[...]).astype(BF16)
        out = mm(rows, weight[layer])
        if d == 0:
            keep_ref[...] = out
        else:
            (s1, s2, s3)[d - 1][...] = out.astype(BF16)


def emission(layer, blocks, capcol, weight):
    width = weight.shape[2]
    part = LIVE // 4
    return call(
        functools.partial(emit_body, layer),
        (jax.ShapeDtypeStruct((part, width), F32),)
        + (jax.ShapeDtypeStruct((part, width), BF16),) * 3,
        [VM] * 10,
        (VM,) * 4,
        "emission",
        1 << 29,
        3 << 20,
        10,
        scratch_shapes=[pltpu.VMEM((GROUPS * CAP, blocks[0].shape[1]), BF16)],
    )(*blocks, capcol, weight)


def last_body(x_ref, x_in, pos_ref, caprow_ref, u0, u1, u2, u3, out, update):
    _, _, y = place_of()
    j = pl.program_id(0)

    @pl.when(j == 0)
    def _():
        gathered(y, (u0, u1, u2, u3), update)

    picked = chosen(caprow_ref[...] - (j * CAP).astype(F32))
    x = (x_ref[j].astype(F32) + mm(picked, update[...])).astype(BF16)
    place = chosen(pos_ref[pl.ds(j, 1), :])
    fresh = mm(place, jnp.concatenate([x, jnp.ones((CAP, 128), BF16)], 1), ((0,), (0,)))
    live = fresh[:, x.shape[1] :] > 0.5
    for at in range(0, x.shape[1], 128):
        old = x_in[0, :, at : at + 128].astype(F32)
        out[0, :, at : at + 128] = jnp.where(live, fresh[:, at : at + 128], old).astype(BF16)


def last_rows(x, x_in, pos, caprow, updates):
    groups, slots, features = x_in.shape
    whole = lambda a: pl.BlockSpec(a.shape, lambda *_: (0,) * a.ndim)
    block = pl.BlockSpec((1, slots, features), lambda i: (i, 0, 0))
    return call(
        last_body,
        jax.ShapeDtypeStruct(x_in.shape, BF16),
        [whole(x), block, whole(pos), whole(caprow)] + [whole(u) for u in updates],
        block,
        "last_rows",
        1 << 30,
        6 << 20,
        12,
        grid=(groups,),
        scratch_shapes=[pltpu.VMEM((LIVE, features), BF16)],
    )(x, x_in, pos, caprow, *updates)


def to_core(a):
    return lax.ppermute(a, "dp", [(i, i ^ 1) for i in range(8)])


def to_x(a, d):
    return lax.ppermute(a, "dp", [(i, (i + 2 * d) % 8) for i in range(8)])


def to_y(a, d):
    return lax.ppermute(a, "tp", [(i, i // 4 * 4 + (i + d) % 4) for i in range(16)])


def to_z(a, d):
    return lax.ppermute(a, "tp", [(i, (i + 4 * d) % 16) for i in range(16)])


def fast(
    spans,
    activation_rows,
    entry_rescale_vector,
    probe_kernel,
    retention_kernel,
    content_kernel,
    valve_kernel,
    retention_minimum,
    extra_attenuation,
    channel_rescale_vector,
    emission_kernel,
    memory_grids,
):
    pos, caprow, capcol = index_maps(spans)
    rows, features = activation_rows.shape
    x_in = activation_rows.reshape(GROUPS, rows // GROUPS, features)
    weights = (probe_kernel, retention_kernel, content_kernel, valve_kernel)
    x, maps, updates, states = x_in, pos, (), None
    for layer in range(BLOCKS):
        own, sent, x = projections(layer, x, maps, updates, entry_rescale_vector, weights)
        keep, *sent = pair_sum(own, to_core(sent))
        got = [to_x(sent[d - 1], d) for d in (1, 2, 3)]
        yields, kk, vv = read_states(
            layer, keep, got, pos, retention_minimum, extra_attenuation,
            channel_rescale_vector, memory_grids,
        )
        states = write_states(layer, kk, vv, memory_grids, states)
        mine = [yields] + [to_x(yields, d) for d in (1, 2, 3)]
        blocks = mine + [to_core(b) for b in mine]
        keep, *sent = emission(layer, blocks, capcol, emission_kernel)
        a, b, c = [to_y(sent[d - 1], d).astype(F32) for d in (1, 2, 3)]
        part = (((keep + a) + b) + c).astype(BF16)
        a, b, c = [to_z(part, d).astype(F32) for d in (1, 2, 3)]
        share = ((part.astype(F32) + b) + (a + c)).astype(BF16)
        updates = [share] + [to_y(share, d) for d in (1, 2, 3)]
        maps = caprow
    mixed = last_rows(x, x_in, pos, caprow, updates)
    return mixed.reshape(rows, features), states


def exchanged(pieces, axis):
    return lax.all_to_all(pieces, axis, split_axis=0, concat_axis=0, tiled=True)


def collect(shard, axis):
    pieces = exchanged(jnp.broadcast_to(shard, (lax.axis_size(axis), *shard.shape)), axis)
    return pieces.reshape(-1, shard.shape[1])


def sum_at_owner(partial, axis):
    count = lax.axis_size(axis)
    pieces = partial.reshape(count, partial.shape[0] // count, partial.shape[1])
    return exchanged(pieces, axis).astype(F32).sum(axis=0)


def general_tick(scores, low, extra, chan, spans, states):
    seqs, heads, dim, _ = states.shape
    query, forget, value, gate = [
        jnp.moveaxis(s.astype(F32).reshape(seqs, SLOTS, heads, dim), 1, 0) for s in scores
    ]
    low = low.reshape(heads, dim)
    query = jax.nn.silu(query)
    decay = jnp.log(low + (1.0 - low) * jax.nn.sigmoid(forget))
    decay = decay + jnp.moveaxis(extra.reshape(seqs, SLOTS, heads), 1, 0)[..., None]
    key = (1.0 - low) * jax.nn.sigmoid(-forget)
    live = jnp.arange(SLOTS)[:, None] < spans[None, :]

    def advance(state, now):
        q, k, a, v, on = now
        fresh = jnp.exp(a)[..., None] * state + k[..., None] * v[..., None, :]
        state = jnp.where(on[:, None, None, None], fresh, state)
        return state, jnp.einsum("shkv,shk->shv", state, q)

    states, read = lax.scan(advance, states, (query, key, decay, value, live))
    read = read * lax.rsqrt(jnp.mean(read * read, axis=-1, keepdims=True) + EPSILON)
    read = read * chan.reshape(heads, dim) * jax.nn.silu(gate)
    read = jnp.where(live[:, :, None, None], read, 0.0)
    return jnp.moveaxis(read, 0, 1).reshape(seqs * SLOTS, heads * dim).astype(BF16), states


def general(
    fresh_spans,
    activation_rows,
    entry_rescale_vector,
    probe_kernel,
    retention_kernel,
    content_kernel,
    valve_kernel,
    retention_minimum,
    extra_attenuation,
    channel_rescale_vector,
    emission_kernel,
    memory_grids,
):
    groups = lax.axis_size("dp")
    rows = activation_rows.shape[0] // groups

    def block(current, layer):
        gain, q, f, v, g, low, extra, chan, out, states = layer
        squares = lax.psum(jnp.sum(current * current, axis=1), "dp")
        scale = lax.rsqrt(squares / D + EPSILON)
        normed = (current * gain).astype(BF16)
        partial = jnp.concatenate(
            [jnp.dot(normed, w, preferred_element_type=F32).astype(BF16) for w in (q, f, v, g)], axis=1
        )
        own = lax.dynamic_slice_in_dim(scale, lax.axis_index("dp") * rows, rows, 0)
        scaled = (sum_at_owner(partial, "dp") * own[:, None]).astype(BF16)
        yields, states = general_tick(
            jnp.split(scaled, 4, axis=1), low, extra, chan, fresh_spans, states
        )
        partial = jnp.dot(collect(yields, "dp"), out, preferred_element_type=F32).astype(BF16)
        update = collect(sum_at_owner(partial, "tp").astype(BF16), "tp")
        return (current + update.astype(F32)).astype(BF16).astype(F32), states

    mixed, states = lax.scan(
        block,
        activation_rows.astype(F32),
        (
            entry_rescale_vector,
            probe_kernel,
            retention_kernel,
            content_kernel,
            valve_kernel,
            retention_minimum,
            extra_attenuation,
            channel_rescale_vector,
            emission_kernel,
            memory_grids,
        ),
    )
    return mixed.astype(BF16), states


def local(activation_rows, fresh_spans, *rest):
    mine = lax.axis_index("dp") == jnp.arange(GROUPS)[:, None]
    spans = lax.psum(jnp.where(mine, fresh_spans.astype(F32)[None, :], 0.0), "dp")
    fits = jnp.max(jnp.sum(spans, axis=1)) <= CAP
    return lax.cond(
        fits,
        lambda spans, mine, *args: fast(spans, *args),
        lambda spans, mine, *args: general(mine, *args),
        spans,
        fresh_spans,
        activation_rows,
        *rest,
    )


def solution(mesh):
    placed = (
        P(None, "dp"),
        P("dp"),
        P(None, "dp"),
        P(None, "dp", "tp"),
        P(None, "dp", "tp"),
        P(None, "dp", "tp"),
        P(None, "dp", "tp"),
        P(None, "tp"),
        P(None, "dp", "tp"),
        P(None, "tp"),
        P(None, "tp", "dp"),
        P(None, "dp", "tp", None, None),
    )
    return jax.shard_map(
        local,
        mesh=mesh,
        in_specs=placed,
        out_specs=(P(None, "dp"), P(None, "dp", "tp", None, None)),
        check_vma=False,
    )
```

```python
import functools

import jax
import jax.numpy as jnp
from jax import lax
from jax.experimental import pallas as pl
from jax.experimental.pallas import tpu as pltpu
from jax.sharding import PartitionSpec as P

D = 4096
BLOCKS = 2
EPSILON = 1e-05
GROUPS = 8
CAP = 128
LIVE = 768
SLOTS = 8
TINY = 1.2e-38
F32 = jnp.float32
BF16 = jnp.bfloat16
VM = pl.BlockSpec(memory_space=pltpu.VMEM)


def iota(shape, dim):
    return lax.broadcasted_iota(jnp.int32, shape, dim)


def mm(a, b, dims=((1,), (0,)), **kw):
    return lax.dot_general(a, b, (dims, ((), ())), preferred_element_type=F32, **kw)


def call(body, out_shape, in_specs, out_specs, name, flops=0, moved=0, vmem=16, **kw):
    return pl.pallas_call(
        body,
        out_shape=out_shape,
        in_specs=in_specs,
        out_specs=out_specs,
        name=name,
        cost_estimate=pl.CostEstimate(flops=flops, bytes_accessed=moved, transcendentals=0),
        compiler_params=pltpu.CompilerParams(vmem_limit_bytes=vmem << 20),
        **kw,
    )


def place_of():
    tp, dp = lax.axis_index("tp"), lax.axis_index("dp")
    core = dp % 2
    return core, dp // 2, jnp.where(core == 0, tp % 4, tp // 4)


def index_body(spans_ref, pos_ref, caprow_ref, capcol_ref):
    total = spans_ref.shape[1]
    seqs = total // GROUPS
    rows = seqs * SLOTS
    row = spans_ref[...].astype(F32)
    spans = jnp.where(iota((GROUPS, total), 1) // seqs == iota((GROUPS, total), 0), row, 0.0)
    at, slot = iota((total, rows), 0) % seqs, iota((total, rows), 1) // SLOTS
    start = mm(spans, (at < slot).astype(F32))
    span = mm(spans, (at == slot).astype(F32))
    slot = (iota((GROUPS, rows), 1) % SLOTS).astype(F32)
    pos_ref[...] = jnp.where(slot < span, start + slot, -1.0)
    count_col = jnp.sum(spans, axis=1, keepdims=True)
    upto = (iota((GROUPS, GROUPS), 1) <= iota((GROUPS, GROUPS), 0)).astype(F32)
    member = (iota((GROUPS, total), 1) // seqs == iota((GROUPS, total), 0)).astype(F32)
    count_row = mm(jnp.broadcast_to(row, (GROUPS, total)), member, ((1,), (1,)))
    end_col = mm(upto, jnp.broadcast_to(count_col, (GROUPS, 128)))[:, :1]
    end_row = mm(count_row, upto, ((1,), (1,)))[:1]
    g = iota((GROUPS, LIVE), 1).astype(F32)
    caprow_ref[...] = g[:1] + jnp.sum(
        jnp.where(g >= end_col, CAP - count_col, 0.0), axis=0, keepdims=True
    )
    g = iota((LIVE, GROUPS), 0).astype(F32)
    cap = g[:, :1] + jnp.sum(
        jnp.where(g >= end_row, CAP - count_row[:1], 0.0), axis=1, keepdims=True
    )
    capcol_ref[...] = jnp.broadcast_to(cap, (LIVE, 128))


def index_maps(spans):
    rows = spans.shape[0] // GROUPS * SLOTS
    return call(
        index_body,
        (
            jax.ShapeDtypeStruct((GROUPS, rows), F32),
            jax.ShapeDtypeStruct((1, LIVE), F32),
            jax.ShapeDtypeStruct((LIVE, 128), F32),
        ),
        [VM],
        (VM, VM, VM),
        "index_maps",
        1 << 20,
        1 << 20,
        4,
    )(spans.reshape(1, -1))


def chosen(pos_row, cap=CAP):
    shape = (cap, pos_row.shape[1])
    return (iota(shape, 0).astype(F32) == pos_row).astype(BF16)


def project(x, layer, gain_ref, weights, out_ref, at):
    normed = (x * gain_ref[layer : layer + 1, :]).astype(BF16)
    width = weights[0].shape[2]
    for n, weight in enumerate(weights):
        out_ref[at, :CAP, n * width : (n + 1) * width] = mm(normed, weight[layer]).astype(BF16)
    squares = x * x
    squares = sum(squares[:, n : n + CAP] for n in range(0, x.shape[1], CAP))
    ones = jnp.ones((8, CAP), BF16)
    high = squares.astype(BF16)
    low = (squares - high.astype(F32)).astype(BF16)
    squares = mm(ones, high, ((1,), (1,))) + mm(ones, low, ((1,), (1,)))
    high = squares.astype(BF16)
    low = (squares - high.astype(F32)).astype(BF16)
    out_ref[at, CAP:, :] = jnp.zeros((8, out_ref.shape[2]), BF16)
    out_ref[at, CAP:, :CAP] = high
    out_ref[at, CAP:, CAP : 2 * CAP] = low


def first_body(layer, x_ref, pos_ref, gain_ref, *refs):
    weights, (own_ref, sent_ref, x_out) = refs[:4], refs[4:]
    core, _, _ = place_of()

    def step(i, _):
        for side, out_ref in ((1, sent_ref), (0, own_ref)):
            j = 2 * i + (1 - core if side else core)
            x = mm(chosen(pos_ref[pl.ds(j, 1), :]), x_ref[j])
            x_out[j] = x.astype(BF16)
            project(x, layer, gain_ref, weights, out_ref, i)
        return 0

    lax.fori_loop(0, 4, step, 0)


def gathered(y, updates, update):
    part = updates[0].shape[0]
    for d, u in enumerate(updates):
        update[pl.ds(pl.multiple_of(((y + 4 - d) % 4) * part, part), part), :] = u[...]


def next_body(layer, x_ref, caprow_ref, u0, u1, u2, u3, gain_ref, *refs):
    weights, (own_ref, sent_ref, x_out, update) = refs[:4], refs[4:]
    core, _, y = place_of()
    gathered(y, (u0, u1, u2, u3), update)

    def step(i, _):
        for side, out_ref in ((1, sent_ref), (0, own_ref)):
            j = 2 * i + (1 - core if side else core)
            picked = chosen(caprow_ref[...] - (j * CAP).astype(F32))
            x = (x_ref[j].astype(F32) + mm(picked, update[...])).astype(BF16)
            x_out[j] = x
            project(x.astype(F32), layer, gain_ref, weights, out_ref, i)
        return 0

    lax.fori_loop(0, 4, step, 0)


def projections(layer, x, maps, updates, gain, weights):
    features = x.shape[-1]
    width = 4 * weights[0].shape[2]
    args = [x, maps, *updates, gain, *weights]
    return call(
        functools.partial(next_body if updates else first_body, layer),
        (
            jax.ShapeDtypeStruct((4, CAP + 8, width), BF16),
            jax.ShapeDtypeStruct((4, CAP + 8, width), BF16),
            jax.ShapeDtypeStruct((GROUPS, CAP, features), BF16),
        ),
        [VM] * len(args),
        (VM,) * 3,
        "next_projection" if updates else "first_projection",
        2 << 30,
        6 << 20,
        scratch_shapes=[pltpu.VMEM((LIVE, features), BF16)] if updates else [],
    )(*args)


def pair_body(own_ref, got_ref, keep_ref, *sent):
    _, x, _ = place_of()

    def step(d, keep):
        at = (x + d) % 4
        squares = own_ref[at, CAP:, : 2 * CAP].astype(F32) + got_ref[at, CAP:, : 2 * CAP].astype(F32)
        squares = squares[:, :CAP] + squares[:, CAP:]
        high = squares if keep else squares.astype(BF16)
        low = squares - high.astype(F32)
        out = keep_ref if keep else sent[d - 1]
        kind = out.dtype
        out[CAP:, :CAP] = high.astype(kind)
        out[CAP:, CAP : 2 * CAP] = low.astype(kind)
        for n in range(0, own_ref.shape[2], 256):
            piece = own_ref[at, :CAP, n : n + 256].astype(F32) + got_ref[at, :CAP, n : n + 256].astype(F32)
            out[:CAP, n : n + 256] = piece.astype(kind)
        out[CAP:, 2 * CAP :] = jnp.zeros((8, own_ref.shape[2] - 2 * CAP), kind)

    for d in (2, 1, 3, 0):
        step(d, d == 0)


def pair_sum(own, got):
    rows, width = own.shape[1:]
    return call(
        pair_body,
        (jax.ShapeDtypeStruct((rows, width), F32),)
        + (jax.ShapeDtypeStruct((rows, width), BF16),) * 3,
        [VM, VM],
        (VM,) * 4,
        "pair_sum",
        1 << 20,
        4 << 20,
        8,
    )(own, got)


def roll_slots(x, d):
    return pltpu.roll(x, d, 1) if d else x


def read_body(layer, keep, r1, r2, r3, pos_ref, low_ref, extra_ref, chan_ref, states, *refs):
    out_rows, kk, vv, held, wide, alive, qa, reads, gates, sems = refs
    heads = kk.shape[0]
    seqs = kk.shape[1]
    rows = seqs * SLOTS
    dim = 128
    parts = sems.shape[0]
    each = seqs // parts

    def fetch(n):
        return pltpu.make_async_copy(
            states.at[layer, pl.ds(n * each, each)], held.at[pl.ds(n * each, each)], sems.at[n]
        )

    for n in range(parts):
        fetch(n).start()
    total = keep[...] + r1[...].astype(F32) + r2[...].astype(F32) + r3[...].astype(F32)
    squares = total[CAP : CAP + 1, :CAP] + total[CAP : CAP + 1, CAP : 2 * CAP]
    scale = lax.rsqrt(squares / D + EPSILON)
    eye = iota((CAP, CAP), 0) == iota((CAP, CAP), 1)
    scale = jnp.sum(jnp.where(eye, scale, 0.0), axis=1, keepdims=True)
    scaled = (total[:CAP] * scale).astype(BF16)
    picked = chosen(pos_ref[pl.ds(lax.axis_index("dp"), 1), :])
    wide[...] = mm(picked, scaled, ((0,), (0,)))
    alive[...] = mm(picked, jnp.ones((CAP, dim), BF16), ((0,), (0,)))
    some = 8
    chunk = some * SLOTS
    shape = (some, SLOTS, dim)

    def prepare(n, _):
        h, c = n // (seqs // some), n % (seqs // some)
        at = pl.ds(pl.multiple_of(c * chunk, chunk), chunk)
        here = pl.ds(c * some, some)

        def part(k):
            lanes = pl.ds(pl.multiple_of((k * heads + h) * dim, dim), dim)
            return wide[at, lanes].reshape(shape)

        lanes = pl.ds(pl.multiple_of(h * dim, dim), dim)
        low = low_ref[layer : layer + 1, lanes]
        chan = chan_ref[layer : layer + 1, lanes]
        both = extra_ref[layer, at, :]
        extra = jnp.sum(jnp.where(iota(both.shape, 1) == h, both, 0.0), axis=1, keepdims=True)
        live = alive[at, :].reshape(shape) > 0.5
        slot = iota(shape, 1)
        query = jax.nn.silu(part(0))
        forget = part(1)
        left = low + (1.0 - low) * jax.nn.sigmoid(forget)
        key = jnp.where(live, (1.0 - low) * jax.nn.sigmoid(-forget), 0.0)
        value = part(2)
        decay = jnp.log(jnp.maximum(left, TINY)) + jnp.broadcast_to(extra, (chunk, dim)).reshape(shape)
        decay = jnp.where(live, decay, 0.0)
        for d in (1, 2, 4):
            decay = decay + jnp.where(slot >= d, roll_slots(decay, d), 0.0)
        ones = jnp.ones((dim, dim), BF16)
        read = jnp.zeros(shape, F32)
        for d in range(SLOTS):
            term = query * roll_slots(key, d)
            if d:
                fade = jnp.exp(jnp.minimum(decay - roll_slots(decay, d), 0.0))
                term = jnp.where(slot >= d, term * fade, 0.0)
            weight = mm(term.astype(BF16).reshape(chunk, dim), ones)
            read = read + weight.reshape(shape) * roll_slots(value, d)
        reads[h, here] = read
        qa[h, here] = (query * jnp.exp(decay)).astype(BF16)
        last = decay[:, SLOTS - 1 :, :]
        whole = jnp.exp(last)
        high = whole.astype(BF16).astype(F32)
        tail = jnp.where(slot == 0, high, jnp.where(slot == 1, whole - high, 0.0))
        kk[h, here, :SLOTS, :] = (key * jnp.exp(last - decay)).astype(BF16)
        kk[h, here, SLOTS:, :] = tail.astype(BF16)
        vv[h, here] = value.astype(BF16)
        gates[h, here] = jax.nn.silu(part(3)) * chan
        return 0

    lax.fori_loop(0, heads * (seqs // some), prepare, 0)

    def apply(n, _):
        fetch(n).wait()
        for s in range(each):
            at = n * each + s
            for h in range(heads):
                reads[h, at] += mm(qa[h, at], held[at, h].astype(BF16))
        return 0

    lax.fori_loop(0, parts, apply, 0)
    for h in range(heads):
        read = reads[h]
        mean = jnp.mean(read * read, axis=-1, keepdims=True)
        head = (read * lax.rsqrt(mean + EPSILON) * gates[h]).astype(BF16).reshape(rows, dim)
        out_rows[:, h * dim : (h + 1) * dim] = mm(picked, head).astype(BF16)


def read_states(layer, keep, got, pos, low, extra, chan, states):
    _, seqs, heads, dim, _ = states.shape
    return call(
        functools.partial(read_body, layer),
        (
            jax.ShapeDtypeStruct((CAP, heads * dim), BF16),
            jax.ShapeDtypeStruct((heads, seqs, 2 * SLOTS, dim), BF16),
            jax.ShapeDtypeStruct((heads, seqs, SLOTS, dim), BF16),
        ),
        [VM] * 8 + [pl.BlockSpec(memory_space=pl.ANY)],
        (VM,) * 3,
        "read_states",
        1 << 30,
        6 << 20,
        20,
        scratch_shapes=[
            pltpu.VMEM((seqs, heads, dim, dim), F32),
            pltpu.VMEM((seqs * SLOTS, 4 * heads * dim), F32),
            pltpu.VMEM((seqs * SLOTS, dim), F32),
            pltpu.VMEM((heads, seqs, SLOTS, dim), BF16),
            pltpu.VMEM((heads, seqs, SLOTS, dim), F32),
            pltpu.VMEM((heads, seqs, SLOTS, dim), F32),
            pltpu.SemaphoreType.DMA((8,)),
        ],
    )(keep, *got, pos, low, extra, chan, states)


def write_body(kk, vv, state_ref, *refs):
    out_state = refs[-1]
    dim = 128
    zero = jnp.zeros((SLOTS, dim), BF16)
    ones = jnp.ones((SLOTS, dim), BF16)

    def one(s, _):
        for h in range(state_ref.shape[2]):
            state = state_ref[0, s, h]
            values = jnp.concatenate(
                [jnp.concatenate([vv[h, s], zero], 1), jnp.concatenate([zero, ones], 1)], 0
            )
            both = mm(kk[h, s], values, ((0,), (0,)))
            out_state[0, s, h] = both[:, dim:] * state + both[:, :dim]
        return 0

    lax.fori_loop(0, state_ref.shape[1], one, 0)


def write_states(layer, kk, vv, states, written):
    _, seqs, heads, dim, _ = states.shape
    here = 4
    block = pl.BlockSpec((1, here, heads, dim, dim), lambda i: (layer, i, 0, 0, 0))
    small = lambda a: pl.BlockSpec((heads, here, a.shape[2], dim), lambda i: (0, i, 0, 0))
    more = [] if written is None else [written]
    return call(
        write_body,
        jax.ShapeDtypeStruct(states.shape, F32),
        [small(kk), small(vv), block] + [pl.BlockSpec(memory_space=pl.ANY)] * len(more),
        block,
        "write_states",
        10 << 30,
        8 << 20,
        8,
        grid=(seqs // here,),
        input_output_aliases={3: 0} if more else {},
    )(kk, vv, states, *more)


def emit_body(layer, *refs):
    blocks, (cap_ref, weight, keep_ref, s1, s2, s3, held) = refs[:8], refs[8:]
    core, x, y = place_of()
    for side in range(2):
        for d in range(4):
            j = 2 * ((x + 4 - d) % 4) + (1 - core if side else core)
            held[pl.ds(pl.multiple_of(j * CAP, CAP), CAP), :] = blocks[4 * side + d][...]
    part = keep_ref.shape[0]
    lanes = iota((part, GROUPS * CAP), 1).astype(F32)
    for d in (2, 1, 3, 0):
        at = pl.multiple_of(((y + d) % 4) * part, part)
        picked = (cap_ref[pl.ds(at, part), :1] == lanes).astype(BF16)
        rows = mm(picked, held[...]).astype(BF16)
        out = mm(rows, weight[layer])
        if d == 0:
            keep_ref[...] = out
        else:
            (s1, s2, s3)[d - 1][...] = out.astype(BF16)


def emission(layer, blocks, capcol, weight):
    width = weight.shape[2]
    part = LIVE // 4
    return call(
        functools.partial(emit_body, layer),
        (jax.ShapeDtypeStruct((part, width), F32),)
        + (jax.ShapeDtypeStruct((part, width), BF16),) * 3,
        [VM] * 10,
        (VM,) * 4,
        "emission",
        1 << 29,
        3 << 20,
        10,
        scratch_shapes=[pltpu.VMEM((GROUPS * CAP, blocks[0].shape[1]), BF16)],
    )(*blocks, capcol, weight)


def last_body(x_ref, x_in, pos_ref, caprow_ref, u0, u1, u2, u3, out, update):
    _, _, y = place_of()
    j = pl.program_id(0)

    @pl.when(j == 0)
    def _():
        gathered(y, (u0, u1, u2, u3), update)

    picked = chosen(caprow_ref[...] - (j * CAP).astype(F32))
    x = (x_ref[j].astype(F32) + mm(picked, update[...])).astype(BF16)
    place = chosen(pos_ref[pl.ds(j, 1), :])
    fresh = mm(place, jnp.concatenate([x, jnp.ones((CAP, 128), BF16)], 1), ((0,), (0,)))
    live = fresh[:, x.shape[1] :] > 0.5
    for at in range(0, x.shape[1], 128):
        old = x_in[0, :, at : at + 128].astype(F32)
        out[0, :, at : at + 128] = jnp.where(live, fresh[:, at : at + 128], old).astype(BF16)


def last_rows(x, x_in, pos, caprow, updates):
    groups, slots, features = x_in.shape
    whole = lambda a: pl.BlockSpec(a.shape, lambda *_: (0,) * a.ndim)
    block = pl.BlockSpec((1, slots, features), lambda i: (i, 0, 0))
    return call(
        last_body,
        jax.ShapeDtypeStruct(x_in.shape, BF16),
        [whole(x), block, whole(pos), whole(caprow)] + [whole(u) for u in updates],
        block,
        "last_rows",
        1 << 30,
        6 << 20,
        12,
        grid=(groups,),
        scratch_shapes=[pltpu.VMEM((LIVE, features), BF16)],
    )(x, x_in, pos, caprow, *updates)


def to_core(a):
    return lax.ppermute(a, "dp", [(i, i ^ 1) for i in range(8)])


def to_x(a, d):
    return lax.ppermute(a, "dp", [(i, (i + 2 * d) % 8) for i in range(8)])


def along(a, d, second):
    pairs = []
    for i in range(128):
        z, y, rest, core = i // 32, i // 8 % 4, i % 8, i % 2
        if core == second:
            y = (y + d) % 4
        else:
            z = (z + d) % 4
        pairs.append((i, z * 32 + y * 8 + rest))
    return lax.ppermute(a, ("tp", "dp"), pairs)


def fast(
    spans,
    activation_rows,
    entry_rescale_vector,
    probe_kernel,
    retention_kernel,
    content_kernel,
    valve_kernel,
    retention_minimum,
    extra_attenuation,
    channel_rescale_vector,
    emission_kernel,
    memory_grids,
):
    pos, caprow, capcol = index_maps(spans)
    rows, features = activation_rows.shape
    x_in = activation_rows.reshape(GROUPS, rows // GROUPS, features)
    weights = (probe_kernel, retention_kernel, content_kernel, valve_kernel)
    x, maps, updates, states = x_in, pos, (), None
    for layer in range(BLOCKS):
        own, sent, x = projections(layer, x, maps, updates, entry_rescale_vector, weights)
        keep, *sent = pair_sum(own, to_core(sent))
        got = [to_x(sent[d - 1], d) for d in (1, 2, 3)]
        yields, kk, vv = read_states(
            layer, keep, got, pos, retention_minimum, extra_attenuation,
            channel_rescale_vector, memory_grids,
        )
        states = write_states(layer, kk, vv, memory_grids, states)
        mine = [yields] + [to_x(yields, d) for d in (1, 2, 3)]
        blocks = mine + [to_core(b) for b in mine]
        keep, *sent = emission(layer, blocks, capcol, emission_kernel)
        a, b, c = [along(sent[d - 1], d, 0).astype(F32) for d in (1, 2, 3)]
        part = (((keep + a) + b) + c).astype(BF16)
        a, b, c = [along(part, d, 1).astype(F32) for d in (1, 2, 3)]
        share = ((part.astype(F32) + b) + (a + c)).astype(BF16)
        updates = [share] + [along(share, d, 0) for d in (1, 2, 3)]
        maps = caprow
    mixed = last_rows(x, x_in, pos, caprow, updates)
    return mixed.reshape(rows, features), states


def exchanged(pieces, axis):
    return lax.all_to_all(pieces, axis, split_axis=0, concat_axis=0, tiled=True)


def collect(shard, axis):
    pieces = exchanged(jnp.broadcast_to(shard, (lax.axis_size(axis), *shard.shape)), axis)
    return pieces.reshape(-1, shard.shape[1])


def sum_at_owner(partial, axis):
    count = lax.axis_size(axis)
    pieces = partial.reshape(count, partial.shape[0] // count, partial.shape[1])
    return exchanged(pieces, axis).astype(F32).sum(axis=0)


def general_tick(scores, low, extra, chan, spans, states):
    seqs, heads, dim, _ = states.shape
    query, forget, value, gate = [
        jnp.moveaxis(s.astype(F32).reshape(seqs, SLOTS, heads, dim), 1, 0) for s in scores
    ]
    low = low.reshape(heads, dim)
    query = jax.nn.silu(query)
    decay = jnp.log(low + (1.0 - low) * jax.nn.sigmoid(forget))
    decay = decay + jnp.moveaxis(extra.reshape(seqs, SLOTS, heads), 1, 0)[..., None]
    key = (1.0 - low) * jax.nn.sigmoid(-forget)
    live = jnp.arange(SLOTS)[:, None] < spans[None, :]

    def advance(state, now):
        q, k, a, v, on = now
        fresh = jnp.exp(a)[..., None] * state + k[..., None] * v[..., None, :]
        state = jnp.where(on[:, None, None, None], fresh, state)
        return state, jnp.einsum("shkv,shk->shv", state, q)

    states, read = lax.scan(advance, states, (query, key, decay, value, live))
    read = read * lax.rsqrt(jnp.mean(read * read, axis=-1, keepdims=True) + EPSILON)
    read = read * chan.reshape(heads, dim) * jax.nn.silu(gate)
    read = jnp.where(live[:, :, None, None], read, 0.0)
    return jnp.moveaxis(read, 0, 1).reshape(seqs * SLOTS, heads * dim).astype(BF16), states


def general(
    fresh_spans,
    activation_rows,
    entry_rescale_vector,
    probe_kernel,
    retention_kernel,
    content_kernel,
    valve_kernel,
    retention_minimum,
    extra_attenuation,
    channel_rescale_vector,
    emission_kernel,
    memory_grids,
):
    groups = lax.axis_size("dp")
    rows = activation_rows.shape[0] // groups

    def block(current, layer):
        gain, q, f, v, g, low, extra, chan, out, states = layer
        squares = lax.psum(jnp.sum(current * current, axis=1), "dp")
        scale = lax.rsqrt(squares / D + EPSILON)
        normed = (current * gain).astype(BF16)
        partial = jnp.concatenate(
            [jnp.dot(normed, w, preferred_element_type=F32).astype(BF16) for w in (q, f, v, g)], axis=1
        )
        own = lax.dynamic_slice_in_dim(scale, lax.axis_index("dp") * rows, rows, 0)
        scaled = (sum_at_owner(partial, "dp") * own[:, None]).astype(BF16)
        yields, states = general_tick(
            jnp.split(scaled, 4, axis=1), low, extra, chan, fresh_spans, states
        )
        partial = jnp.dot(collect(yields, "dp"), out, preferred_element_type=F32).astype(BF16)
        update = collect(sum_at_owner(partial, "tp").astype(BF16), "tp")
        return (current + update.astype(F32)).astype(BF16).astype(F32), states

    mixed, states = lax.scan(
        block,
        activation_rows.astype(F32),
        (
            entry_rescale_vector,
            probe_kernel,
            retention_kernel,
            content_kernel,
            valve_kernel,
            retention_minimum,
            extra_attenuation,
            channel_rescale_vector,
            emission_kernel,
            memory_grids,
        ),
    )
    return mixed.astype(BF16), states


def local(activation_rows, fresh_spans, *rest):
    count = fresh_spans.shape[0]
    spans = lax.dynamic_update_slice(
        jnp.zeros((GROUPS * count,), jnp.int32), fresh_spans, (lax.axis_index("dp") * count,)
    )
    spans = lax.psum(spans, "dp")
    fits = jnp.max(jnp.sum(spans.reshape(GROUPS, count), axis=1)) <= CAP
    return lax.cond(
        fits,
        lambda spans, mine, *args: fast(spans, *args),
        lambda spans, mine, *args: general(mine, *args),
        spans,
        fresh_spans,
        activation_rows,
        *rest,
    )


def solution(mesh):
    placed = (
        P(None, "dp"),
        P("dp"),
        P(None, "dp"),
        P(None, "dp", "tp"),
        P(None, "dp", "tp"),
        P(None, "dp", "tp"),
        P(None, "dp", "tp"),
        P(None, "tp"),
        P(None, "dp", "tp"),
        P(None, "tp"),
        P(None, "tp", "dp"),
        P(None, "dp", "tp", None, None),
    )
    return jax.shard_map(
        local,
        mesh=mesh,
        in_specs=placed,
        out_specs=(P(None, "dp"), P(None, "dp", "tp", None, None)),
        check_vma=False,
    )
```

```python
import functools

import jax
import jax.numpy as jnp
from jax import lax
from jax.experimental import pallas as pl
from jax.experimental.pallas import tpu as pltpu
from jax.sharding import PartitionSpec as P

D = 4096
BLOCKS = 2
EPSILON = 1e-05
GROUPS = 8
CAP = 128
LIVE = 768
SLOTS = 8
TINY = 1.2e-38
F32 = jnp.float32
BF16 = jnp.bfloat16
VM = pl.BlockSpec(memory_space=pltpu.VMEM)


def iota(shape, dim):
    return lax.broadcasted_iota(jnp.int32, shape, dim)


def mm(a, b, dims=((1,), (0,)), **kw):
    return lax.dot_general(a, b, (dims, ((), ())), preferred_element_type=F32, **kw)


def call(body, out_shape, in_specs, out_specs, name, flops=0, moved=0, vmem=16, **kw):
    return pl.pallas_call(
        body,
        out_shape=out_shape,
        in_specs=in_specs,
        out_specs=out_specs,
        name=name,
        cost_estimate=pl.CostEstimate(flops=flops, bytes_accessed=moved, transcendentals=0),
        compiler_params=pltpu.CompilerParams(vmem_limit_bytes=vmem << 20),
        **kw,
    )


def place_of():
    tp, dp = lax.axis_index("tp"), lax.axis_index("dp")
    core = dp % 2
    return core, dp // 2, jnp.where(core == 0, tp % 4, tp // 4)


def index_body(spans_ref, pos_ref, fits_ref):
    total = spans_ref.shape[1]
    seqs = total // GROUPS
    rows = seqs * SLOTS
    row = spans_ref[...].astype(F32)
    spans = jnp.where(iota((GROUPS, total), 1) // seqs == iota((GROUPS, total), 0), row, 0.0)
    at, slot = iota((total, rows), 0) % seqs, iota((total, rows), 1) // SLOTS
    start = mm(spans, (at < slot).astype(F32))
    span = mm(spans, (at == slot).astype(F32))
    slot = (iota((GROUPS, rows), 1) % SLOTS).astype(F32)
    pos_ref[...] = jnp.where(slot < span, start + slot, -1.0)
    count_col = jnp.sum(spans, axis=1, keepdims=True)
    fits_ref[0] = (jnp.max(count_col) <= CAP).astype(jnp.int32)


def index_maps(spans):
    rows = spans.shape[0] // GROUPS * SLOTS
    return call(
        index_body,
        (
            jax.ShapeDtypeStruct((GROUPS, rows), F32),
            jax.ShapeDtypeStruct((1,), jnp.int32),
        ),
        [VM],
        (VM, pl.BlockSpec(memory_space=pltpu.SMEM)),
        "index_maps",
        1 << 20,
        1 << 20,
        4,
    )(spans.reshape(1, -1))


def cross_body(pos_ref, spread, packed):
    rows = pos_ref.shape[1]
    live = (pos_ref[...] >= 0.0).astype(F32)
    count_col = jnp.sum(live, axis=1, keepdims=True)
    count_row = mm(jnp.ones((GROUPS, rows), F32), live, ((1,), (1,)))
    upto = (iota((GROUPS, GROUPS), 1) <= iota((GROUPS, GROUPS), 0)).astype(F32)
    end_col = mm(upto, jnp.broadcast_to(count_col, (GROUPS, 128)))[:, :1]
    end_row = mm(count_row, upto, ((1,), (1,)))[:1]
    g = iota((GROUPS, LIVE), 1).astype(F32)
    cap_row = g[:1] + jnp.sum(jnp.where(g >= end_col, CAP - count_col, 0.0), axis=0, keepdims=True)
    g = iota((LIVE, GROUPS), 0).astype(F32)
    more = jnp.where(g >= end_row, CAP - count_row[:1], 0.0)
    cap_col = g[:, :1] + jnp.sum(more, axis=1, keepdims=True)
    lanes = iota((LIVE, CAP), 1).astype(F32)
    for j in range(GROUPS):
        at = slice(j * CAP, (j + 1) * CAP)
        spread[at, :] = chosen(cap_row - float(j * CAP))
        packed[:, at] = (cap_col - float(j * CAP) == lanes).astype(BF16)


def cross_maps(pos):
    wide = GROUPS * CAP
    return call(
        cross_body,
        (jax.ShapeDtypeStruct((wide, LIVE), BF16), jax.ShapeDtypeStruct((LIVE, wide), BF16)),
        [VM],
        (VM, VM),
        "cross_maps",
        1 << 28,
        3 << 20,
        6,
    )(pos)


def chosen(pos_row, cap=CAP):
    shape = (cap, pos_row.shape[1])
    return (iota(shape, 0).astype(F32) == pos_row).astype(BF16)


def halves(squares):
    high = squares.astype(BF16)
    return high, (squares - high.astype(F32)).astype(BF16)


def project(x, layer, gain_ref, weights, outs, at):
    normed = (x * gain_ref[layer : layer + 1, :]).astype(BF16)
    width = weights[0].shape[2]
    for n, weight in enumerate(weights):
        found = mm(normed, weight[layer]).astype(BF16)
        for side, out in enumerate(outs):
            out[at, :CAP, n * width : (n + 1) * width] = found[side * CAP : (side + 1) * CAP]
    squares = x * x
    squares = sum(squares[:, n : n + CAP] for n in range(0, x.shape[1], CAP))
    ones = jnp.ones((8, CAP), BF16)
    high, low = halves(squares)
    squares = mm(ones, high, ((1,), (1,))) + mm(ones, low, ((1,), (1,)))
    for side, out in enumerate(outs):
        high, low = halves(squares[:, side * CAP : (side + 1) * CAP])
        out[at, CAP:, :] = jnp.zeros((8, out.shape[2]), BF16)
        out[at, CAP:, :CAP] = high
        out[at, CAP:, CAP : 2 * CAP] = low


def spread_rows(spread, j):
    return spread[pl.ds(pl.multiple_of(j * CAP, CAP), CAP), :]


def pair_at(i):
    core, _, _ = place_of()
    return 2 * i + core, 2 * i + 1 - core


def first_body(layer, x_ref, pos_ref, gain_ref, *refs):
    weights, (own_ref, sent_ref, x_out) = refs[:4], refs[4:]

    def step(i, _):
        rows = [mm(chosen(pos_ref[pl.ds(j, 1), :]), x_ref[j]) for j in pair_at(i)]
        for j, x in zip(pair_at(i), rows):
            x_out[j] = x.astype(BF16)
        project(jnp.concatenate(rows, 0), layer, gain_ref, weights, (own_ref, sent_ref), i)
        return 0

    lax.fori_loop(0, 4, step, 0)


def gathered(y, updates, update):
    part = updates[0].shape[0]
    for d, u in enumerate(updates):
        update[pl.ds(pl.multiple_of(((y + 4 - d) % 4) * part, part), part), :] = u[...]


def next_body(layer, x_ref, spread, u0, u1, u2, u3, gain_ref, *refs):
    weights, (own_ref, sent_ref, x_out, update) = refs[:4], refs[4:]
    _, _, p = place_of()
    gathered(p, (u0, u1, u2, u3), update)

    def step(i, _):
        picked = jnp.concatenate([spread_rows(spread, j) for j in pair_at(i)], 0)
        x = jnp.concatenate([x_ref[j] for j in pair_at(i)], 0)
        x = (x.astype(F32) + mm(picked, update[...])).astype(BF16)
        for side, j in enumerate(pair_at(i)):
            x_out[j] = x[side * CAP : (side + 1) * CAP]
        project(x.astype(F32), layer, gain_ref, weights, (own_ref, sent_ref), i)
        return 0

    lax.fori_loop(0, 4, step, 0)


def projections(layer, x, maps, updates, gain, weights):
    features = x.shape[-1]
    width = 4 * weights[0].shape[2]
    args = [x, maps, *updates, gain, *weights]
    return call(
        functools.partial(next_body if updates else first_body, layer),
        (
            jax.ShapeDtypeStruct((4, CAP + 8, width), BF16),
            jax.ShapeDtypeStruct((4, CAP + 8, width), BF16),
            jax.ShapeDtypeStruct((GROUPS, CAP, features), BF16),
        ),
        [VM] * len(args),
        (VM,) * 3,
        "next_projection" if updates else "first_projection",
        2 << 30,
        6 << 20,
        scratch_shapes=[pltpu.VMEM((LIVE, features), BF16)] if updates else [],
    )(*args)


def pair_body(own_ref, got_ref, keep_ref, *sent):
    _, x, _ = place_of()

    def step(d, keep):
        at = (x + d) % 4
        squares = own_ref[at, CAP:, : 2 * CAP].astype(F32) + got_ref[at, CAP:, : 2 * CAP].astype(F32)
        squares = squares[:, :CAP] + squares[:, CAP:]
        high = squares if keep else squares.astype(BF16)
        low = squares - high.astype(F32)
        out = keep_ref if keep else sent[d - 1]
        kind = out.dtype
        out[CAP:, :CAP] = high.astype(kind)
        out[CAP:, CAP : 2 * CAP] = low.astype(kind)
        for n in range(0, own_ref.shape[2], 256):
            piece = own_ref[at, :CAP, n : n + 256].astype(F32) + got_ref[at, :CAP, n : n + 256].astype(F32)
            out[:CAP, n : n + 256] = piece.astype(kind)
        out[CAP:, 2 * CAP :] = jnp.zeros((8, own_ref.shape[2] - 2 * CAP), kind)

    for d in (2, 1, 3, 0):
        step(d, d == 0)


def pair_sum(own, got):
    rows, width = own.shape[1:]
    return call(
        pair_body,
        (jax.ShapeDtypeStruct((rows, width), F32),)
        + (jax.ShapeDtypeStruct((rows, width), BF16),) * 3,
        [VM, VM],
        (VM,) * 4,
        "pair_sum",
        1 << 20,
        4 << 20,
        8,
    )(own, got)


def roll_slots(x, d):
    return pltpu.roll(x, d, 1) if d else x


def read_body(layer, keep, r1, r2, r3, pos_ref, low_ref, extra_ref, chan_ref, states, *refs):
    out_rows, kk, vv, held, wide, alive, more, qa, reads, gates, sems = refs
    heads = kk.shape[0]
    seqs = kk.shape[1]
    rows = seqs * SLOTS
    dim = 128
    parts = sems.shape[0]
    each = seqs // parts

    def fetch(n):
        return pltpu.make_async_copy(
            states.at[layer, pl.ds(n * each, each)], held.at[pl.ds(n * each, each)], sems.at[n]
        )

    for n in range(parts):
        fetch(n).start()
    total = (keep[...] + r1[...].astype(F32)) + (r2[...].astype(F32) + r3[...].astype(F32))
    squares = total[CAP : CAP + 1, :CAP] + total[CAP : CAP + 1, CAP : 2 * CAP]
    scale = lax.rsqrt(squares / D + EPSILON)
    eye = iota((CAP, CAP), 0) == iota((CAP, CAP), 1)
    scale = jnp.sum(jnp.where(eye, scale, 0.0), axis=1, keepdims=True)
    scaled = (total[:CAP] * scale).astype(BF16)
    picked = chosen(pos_ref[pl.ds(lax.axis_index("dp"), 1), :])
    wide[...] = mm(picked, scaled, ((0,), (0,)))
    alive[...] = mm(picked, jnp.ones((CAP, dim), BF16), ((0,), (0,)))
    for h in range(heads):
        row = extra_ref[layer, h : h + 1, :]
        more[h] = jnp.transpose(jnp.broadcast_to(row, (dim, rows)))
    some = 8
    chunk = some * SLOTS
    shape = (some, SLOTS, dim)

    def prepare(n, _):
        h, c = n // (seqs // some), n % (seqs // some)
        at = pl.ds(pl.multiple_of(c * chunk, chunk), chunk)
        here = pl.ds(c * some, some)

        def part(k):
            lanes = pl.ds(pl.multiple_of((k * heads + h) * dim, dim), dim)
            return wide[at, lanes].reshape(shape)

        lanes = pl.ds(pl.multiple_of(h * dim, dim), dim)
        low = low_ref[layer : layer + 1, lanes]
        chan = chan_ref[layer : layer + 1, lanes]
        extra = more[h, at, :].reshape(shape)
        live = alive[at, :].reshape(shape) > 0.5
        slot = iota(shape, 1)
        query = jax.nn.silu(part(0))
        forget = part(1)
        left = low + (1.0 - low) * jax.nn.sigmoid(forget)
        key = jnp.where(live, (1.0 - low) * jax.nn.sigmoid(-forget), 0.0)
        value = part(2)
        decay = jnp.log(jnp.maximum(left, TINY)) + extra
        decay = jnp.where(live, decay, 0.0)
        for d in (1, 2, 4):
            decay = decay + jnp.where(slot >= d, roll_slots(decay, d), 0.0)
        ones = jnp.ones((dim, dim), BF16)
        read = jnp.zeros(shape, F32)
        for d in range(SLOTS):
            term = query * roll_slots(key, d)
            if d:
                fade = jnp.exp(jnp.minimum(decay - roll_slots(decay, d), 0.0))
                term = jnp.where(slot >= d, term * fade, 0.0)
            weight = mm(term.astype(BF16).reshape(chunk, dim), ones)
            read = read + weight.reshape(shape) * roll_slots(value, d)
        reads[h, here] = read
        qa[h, here] = (query * jnp.exp(decay)).astype(BF16)
        last = decay[:, SLOTS - 1 :, :]
        whole = jnp.exp(last)
        high = whole.astype(BF16).astype(F32)
        tail = jnp.where(slot == 0, high, jnp.where(slot == 1, whole - high, 0.0))
        kk[h, here, :SLOTS, :] = (key * jnp.exp(last - decay)).astype(BF16)
        kk[h, here, SLOTS:, :] = tail.astype(BF16)
        vv[h, here] = value.astype(BF16)
        gates[h, here] = jax.nn.silu(part(3)) * chan
        return 0

    lax.fori_loop(0, heads * (seqs // some), prepare, 0)

    def apply(n, _):
        fetch(n).wait()
        for s in range(each):
            at = n * each + s
            for h in range(heads):
                reads[h, at] += mm(qa[h, at], held[at, h].astype(BF16))
        return 0

    lax.fori_loop(0, parts, apply, 0)
    for h in range(heads):
        read = reads[h]
        mean = jnp.mean(read * read, axis=-1, keepdims=True)
        head = (read * lax.rsqrt(mean + EPSILON) * gates[h]).astype(BF16).reshape(rows, dim)
        out_rows[:, h * dim : (h + 1) * dim] = mm(picked, head).astype(BF16)


def read_states(layer, keep, got, pos, low, extra, chan, states):
    _, seqs, heads, dim, _ = states.shape
    return call(
        functools.partial(read_body, layer),
        (
            jax.ShapeDtypeStruct((CAP, heads * dim), BF16),
            jax.ShapeDtypeStruct((heads, seqs, 2 * SLOTS, dim), BF16),
            jax.ShapeDtypeStruct((heads, seqs, SLOTS, dim), BF16),
        ),
        [VM] * 8 + [pl.BlockSpec(memory_space=pl.ANY)],
        (VM,) * 3,
        "read_states",
        1 << 30,
        6 << 20,
        20,
        scratch_shapes=[
            pltpu.VMEM((seqs, heads, dim, dim), F32),
            pltpu.VMEM((seqs * SLOTS, 4 * heads * dim), F32),
            pltpu.VMEM((seqs * SLOTS, dim), F32),
            pltpu.VMEM((heads, seqs * SLOTS, dim), F32),
            pltpu.VMEM((heads, seqs, SLOTS, dim), BF16),
            pltpu.VMEM((heads, seqs, SLOTS, dim), F32),
            pltpu.VMEM((heads, seqs, SLOTS, dim), F32),
            pltpu.SemaphoreType.DMA((8,)),
        ],
    )(keep, *got, pos, low, jnp.swapaxes(extra, 1, 2), chan, states)


def write_body(kk, vv, state_ref, *refs):
    out_state = refs[-1]
    dim = 128
    zero = jnp.zeros((SLOTS, dim), BF16)
    ones = jnp.ones((SLOTS, dim), BF16)

    def one(s, _):
        for h in range(state_ref.shape[2]):
            state = state_ref[0, s, h]
            values = jnp.concatenate(
                [jnp.concatenate([vv[h, s], zero], 1), jnp.concatenate([zero, ones], 1)], 0
            )
            both = mm(kk[h, s], values, ((0,), (0,)))
            out_state[0, s, h] = both[:, dim:] * state + both[:, :dim]
        return 0

    lax.fori_loop(0, state_ref.shape[1], one, 0)


def write_states(layer, half, kk, vv, states, written):
    _, seqs, heads, dim, _ = states.shape
    here = 4
    first = half * (seqs // here // 2)
    block = pl.BlockSpec((1, here, heads, dim, dim), lambda i: (layer, first + i, 0, 0, 0))
    small = lambda a: pl.BlockSpec((heads, here, a.shape[2], dim), lambda i: (0, first + i, 0, 0))
    more = [] if written is None else [written]
    return call(
        write_body,
        jax.ShapeDtypeStruct(states.shape, F32),
        [small(kk), small(vv), block] + [pl.BlockSpec(memory_space=pl.ANY)] * len(more),
        block,
        "write_states",
        5 << 30,
        4 << 20,
        8,
        grid=(seqs // here // 2,),
        input_output_aliases={3: 0} if more else {},
    )(kk, vv, states, *more)


def emit_body(layer, *refs):
    blocks, (packed, weight, keep_ref, s1, s2, s3, held) = refs[:8], refs[8:]
    core, x, y = place_of()
    for side in range(2):
        for d in range(4):
            j = 2 * ((x + 4 - d) % 4) + (1 - core if side else core)
            held[pl.ds(pl.multiple_of(j * CAP, CAP), CAP), :] = blocks[4 * side + d][...]
    part = keep_ref.shape[0]
    for d in (2, 1, 3, 0):
        at = pl.multiple_of(((y + d) % 4) * part, part)
        rows = mm(packed[pl.ds(at, part), :], held[...]).astype(BF16)
        out = mm(rows, weight[layer])
        if d == 0:
            keep_ref[...] = out
        else:
            (s1, s2, s3)[d - 1][...] = out.astype(BF16)


def emission(layer, blocks, packed, weight):
    width = weight.shape[2]
    part = LIVE // 4
    return call(
        functools.partial(emit_body, layer),
        (jax.ShapeDtypeStruct((part, width), F32),)
        + (jax.ShapeDtypeStruct((part, width), BF16),) * 3,
        [VM] * 10,
        (VM,) * 4,
        "emission",
        1 << 29,
        3 << 20,
        10,
        scratch_shapes=[pltpu.VMEM((GROUPS * CAP, blocks[0].shape[1]), BF16)],
    )(*blocks, packed, weight)


def dead_body(x_in, pos_ref, out):
    place = chosen(pos_ref[pl.ds(pl.program_id(0), 1), :])
    live = mm(place, jnp.ones((CAP, 128), BF16), ((0,), (0,))) > 0.5
    for at in range(0, x_in.shape[2], 128):
        old = x_in[0, :, at : at + 128].astype(F32)
        out[0, :, at : at + 128] = jnp.where(live, 0.0, old).astype(BF16)


def dead_rows(x_in, pos):
    groups, slots, features = x_in.shape
    block = pl.BlockSpec((1, slots, features), lambda i: (i, 0, 0))
    return call(
        dead_body,
        jax.ShapeDtypeStruct(x_in.shape, BF16),
        [block, pl.BlockSpec(pos.shape, lambda i: (0, 0))],
        block,
        "dead_rows",
        1 << 28,
        4 << 20,
        6,
        grid=(groups,),
    )(x_in, pos)


def last_body(x_all, dead, pos_ref, spread, u0, u1, u2, u3, out, update, fresh_x):
    step = pl.program_id(0)

    @pl.when(step == 0)
    def _():
        _, _, p = place_of()
        gathered(p, (u0, u1, u2, u3), update)

        def apply(i, _):
            picked = jnp.concatenate([spread_rows(spread, j) for j in pair_at(i)], 0)
            x = jnp.concatenate([x_all[j] for j in pair_at(i)], 0)
            x = (x.astype(F32) + mm(picked, update[...])).astype(BF16)
            for side, j in enumerate(pair_at(i)):
                fresh_x[j] = x[side * CAP : (side + 1) * CAP]
            return 0

        lax.fori_loop(0, 4, apply, 0)

    place = chosen(pos_ref[pl.ds(step, 1), :])
    fresh = mm(place, fresh_x[step], ((0,), (0,))).astype(BF16)
    out[0] = fresh + dead[step]


def last_rows(x_all, dead, pos, spread, updates):
    groups, slots, features = dead.shape
    whole = lambda a: pl.BlockSpec(a.shape, lambda *_: (0,) * a.ndim)
    return call(
        last_body,
        jax.ShapeDtypeStruct(dead.shape, BF16),
        [whole(a) for a in (x_all, dead, pos, spread, *updates)],
        pl.BlockSpec((1, slots, features), lambda i: (i, 0, 0)),
        "last_rows",
        1 << 30,
        6 << 20,
        16,
        grid=(groups,),
        scratch_shapes=[pltpu.VMEM((LIVE, features), BF16), pltpu.VMEM((GROUPS, CAP, features), BF16)],
    )(x_all, dead, pos, spread, *updates)


def to_core(a):
    return lax.ppermute(a, "dp", [(i, i ^ 1) for i in range(8)])


def to_x(a, d):
    return lax.ppermute(a, "dp", [(i, (i + 2 * d) % 8) for i in range(8)])


def along(a, d, second):
    pairs = []
    for i in range(128):
        z, y, rest, core = i // 32, i // 8 % 4, i % 8, i % 2
        if core == second:
            y = (y + d) % 4
        else:
            z = (z + d) % 4
        pairs.append((i, z * 32 + y * 8 + rest))
    return lax.ppermute(a, ("tp", "dp"), pairs)


def fast(
    pos,
    activation_rows,
    entry_rescale_vector,
    probe_kernel,
    retention_kernel,
    content_kernel,
    valve_kernel,
    retention_minimum,
    extra_attenuation,
    channel_rescale_vector,
    emission_kernel,
    memory_grids,
):
    spread, packed = cross_maps(pos)
    rows, features = activation_rows.shape
    x_in = activation_rows.reshape(GROUPS, rows // GROUPS, features)
    weights = (probe_kernel, retention_kernel, content_kernel, valve_kernel)
    dead = dead_rows(x_in, pos)
    x, maps, updates, states = x_in, pos, (), None
    for layer in range(BLOCKS):
        own, sent, x = projections(layer, x, maps, updates, entry_rescale_vector, weights)
        keep, *sent = pair_sum(own, to_core(sent))
        got = [to_x(sent[d - 1], d) for d in (1, 2, 3)]
        yields, kk, vv = read_states(
            layer, keep, got, pos, retention_minimum, extra_attenuation,
            channel_rescale_vector, memory_grids,
        )
        states = write_states(layer, 0, kk, vv, memory_grids, states)
        mine = [yields] + [to_x(yields, d) for d in (1, 2, 3)]
        blocks = mine + [to_core(b) for b in mine]
        keep, *sent = emission(layer, blocks, packed, emission_kernel)
        a, b, c = [along(sent[d - 1], d, 0).astype(F32) for d in (1, 2, 3)]
        part = (((keep + a) + b) + c).astype(BF16)
        part, states = lax.optimization_barrier((part, states))
        states = write_states(layer, 1, kk, vv, memory_grids, states)
        a, b, c = [along(part, d, 1).astype(F32) for d in (1, 2, 3)]
        share = ((part.astype(F32) + b) + (a + c)).astype(BF16)
        share, states = lax.optimization_barrier((share, states))
        updates = [share] + [along(share, d, 0) for d in (1, 2, 3)]
        if layer == 0:
            dead, *updates = lax.optimization_barrier((dead, *updates))
        maps = spread
    mixed = last_rows(x, dead, pos, spread, updates)
    return mixed.reshape(rows, features), states


def exchanged(pieces, axis):
    return lax.all_to_all(pieces, axis, split_axis=0, concat_axis=0, tiled=True)


def collect(shard, axis):
    pieces = exchanged(jnp.broadcast_to(shard, (lax.axis_size(axis), *shard.shape)), axis)
    return pieces.reshape(-1, shard.shape[1])


def sum_at_owner(partial, axis):
    count = lax.axis_size(axis)
    pieces = partial.reshape(count, partial.shape[0] // count, partial.shape[1])
    return exchanged(pieces, axis).astype(F32).sum(axis=0)


def general_tick(scores, low, extra, chan, spans, states):
    seqs, heads, dim, _ = states.shape
    query, forget, value, gate = [
        jnp.moveaxis(s.astype(F32).reshape(seqs, SLOTS, heads, dim), 1, 0) for s in scores
    ]
    low = low.reshape(heads, dim)
    query = jax.nn.silu(query)
    decay = jnp.log(low + (1.0 - low) * jax.nn.sigmoid(forget))
    decay = decay + jnp.moveaxis(extra.reshape(seqs, SLOTS, heads), 1, 0)[..., None]
    key = (1.0 - low) * jax.nn.sigmoid(-forget)
    live = jnp.arange(SLOTS)[:, None] < spans[None, :]

    def advance(state, now):
        q, k, a, v, on = now
        fresh = jnp.exp(a)[..., None] * state + k[..., None] * v[..., None, :]
        state = jnp.where(on[:, None, None, None], fresh, state)
        return state, jnp.einsum("shkv,shk->shv", state, q)

    states, read = lax.scan(advance, states, (query, key, decay, value, live))
    read = read * lax.rsqrt(jnp.mean(read * read, axis=-1, keepdims=True) + EPSILON)
    read = read * chan.reshape(heads, dim) * jax.nn.silu(gate)
    read = jnp.where(live[:, :, None, None], read, 0.0)
    return jnp.moveaxis(read, 0, 1).reshape(seqs * SLOTS, heads * dim).astype(BF16), states


def general(
    fresh_spans,
    activation_rows,
    entry_rescale_vector,
    probe_kernel,
    retention_kernel,
    content_kernel,
    valve_kernel,
    retention_minimum,
    extra_attenuation,
    channel_rescale_vector,
    emission_kernel,
    memory_grids,
):
    groups = lax.axis_size("dp")
    rows = activation_rows.shape[0] // groups

    def block(current, layer):
        gain, q, f, v, g, low, extra, chan, out, states = layer
        squares = lax.psum(jnp.sum(current * current, axis=1), "dp")
        scale = lax.rsqrt(squares / D + EPSILON)
        normed = (current * gain).astype(BF16)
        partial = jnp.concatenate(
            [jnp.dot(normed, w, preferred_element_type=F32).astype(BF16) for w in (q, f, v, g)], axis=1
        )
        own = lax.dynamic_slice_in_dim(scale, lax.axis_index("dp") * rows, rows, 0)
        scaled = (sum_at_owner(partial, "dp") * own[:, None]).astype(BF16)
        yields, states = general_tick(
            jnp.split(scaled, 4, axis=1), low, extra, chan, fresh_spans, states
        )
        partial = jnp.dot(collect(yields, "dp"), out, preferred_element_type=F32).astype(BF16)
        update = collect(sum_at_owner(partial, "tp").astype(BF16), "tp")
        return (current + update.astype(F32)).astype(BF16).astype(F32), states

    mixed, states = lax.scan(
        block,
        activation_rows.astype(F32),
        (
            entry_rescale_vector,
            probe_kernel,
            retention_kernel,
            content_kernel,
            valve_kernel,
            retention_minimum,
            extra_attenuation,
            channel_rescale_vector,
            emission_kernel,
            memory_grids,
        ),
    )
    return mixed.astype(BF16), states


def local(activation_rows, fresh_spans, *rest):
    count = fresh_spans.shape[0]
    spans = lax.dynamic_update_slice(
        jnp.zeros((GROUPS * count,), jnp.int32), fresh_spans, (lax.axis_index("dp") * count,)
    )
    spans = lax.psum(spans, "dp")
    pos, fits = index_maps(spans)
    return lax.cond(
        fits[0] > 0,
        lambda: fast(pos, activation_rows, *rest),
        lambda: general(fresh_spans, activation_rows, *rest),
    )


def solution(mesh):
    placed = (
        P(None, "dp"),
        P("dp"),
        P(None, "dp"),
        P(None, "dp", "tp"),
        P(None, "dp", "tp"),
        P(None, "dp", "tp"),
        P(None, "dp", "tp"),
        P(None, "tp"),
        P(None, "dp", "tp"),
        P(None, "tp"),
        P(None, "tp", "dp"),
        P(None, "dp", "tp", None, None),
    )
    return jax.shard_map(
        local,
        mesh=mesh,
        in_specs=placed,
        out_specs=(P(None, "dp"), P(None, "dp", "tp", None, None)),
        check_vma=False,
    )
```

```python
import functools

import jax
import jax.numpy as jnp
from jax import lax
from jax.experimental import pallas as pl
from jax.experimental.pallas import tpu as pltpu
from jax.sharding import PartitionSpec as P

D = 4096
BLOCKS = 2
EPSILON = 1e-05
GROUPS = 8
CAP = 128
LIVE = 768
SLOTS = 8
TINY = 1.2e-38
F32 = jnp.float32
BF16 = jnp.bfloat16
VM = pl.BlockSpec(memory_space=pltpu.VMEM)


def iota(shape, dim):
    return lax.broadcasted_iota(jnp.int32, shape, dim)


def mm(a, b, dims=((1,), (0,)), **kw):
    return lax.dot_general(a, b, (dims, ((), ())), preferred_element_type=F32, **kw)


def call(body, out_shape, in_specs, out_specs, name, flops=0, moved=0, vmem=16, **kw):
    return pl.pallas_call(
        body,
        out_shape=out_shape,
        in_specs=in_specs,
        out_specs=out_specs,
        name=name,
        cost_estimate=pl.CostEstimate(flops=flops, bytes_accessed=moved, transcendentals=0),
        compiler_params=pltpu.CompilerParams(vmem_limit_bytes=vmem << 20),
        **kw,
    )


def place_of():
    tp, dp = lax.axis_index("tp"), lax.axis_index("dp")
    core = dp % 2
    return core, dp // 2, jnp.where(core == 0, tp % 4, tp // 4)


def index_body(spans_ref, pos_ref, fits_ref):
    total = spans_ref.shape[1]
    seqs = total // GROUPS
    rows = seqs * SLOTS
    row = spans_ref[...].astype(F32)
    spans = jnp.where(iota((GROUPS, total), 1) // seqs == iota((GROUPS, total), 0), row, 0.0)
    at, slot = iota((total, rows), 0) % seqs, iota((total, rows), 1) // SLOTS
    start = mm(spans, (at < slot).astype(F32))
    span = mm(spans, (at == slot).astype(F32))
    slot = (iota((GROUPS, rows), 1) % SLOTS).astype(F32)
    pos_ref[...] = jnp.where(slot < span, start + slot, -1.0)
    count_col = jnp.sum(spans, axis=1, keepdims=True)
    fits_ref[0] = (jnp.max(count_col) <= CAP).astype(jnp.int32)


def index_maps(spans):
    rows = spans.shape[0] // GROUPS * SLOTS
    return call(
        index_body,
        (
            jax.ShapeDtypeStruct((GROUPS, rows), F32),
            jax.ShapeDtypeStruct((1,), jnp.int32),
        ),
        [VM],
        (VM, pl.BlockSpec(memory_space=pltpu.SMEM)),
        "index_maps",
        1 << 20,
        1 << 20,
        4,
    )(spans.reshape(1, -1))


def cross_body(pos_ref, spread, packed):
    rows = pos_ref.shape[1]
    live = (pos_ref[...] >= 0.0).astype(F32)
    count_col = jnp.sum(live, axis=1, keepdims=True)
    count_row = mm(jnp.ones((GROUPS, rows), F32), live, ((1,), (1,)))
    upto = (iota((GROUPS, GROUPS), 1) <= iota((GROUPS, GROUPS), 0)).astype(F32)
    end_col = mm(upto, jnp.broadcast_to(count_col, (GROUPS, 128)))[:, :1]
    end_row = mm(count_row, upto, ((1,), (1,)))[:1]
    g = iota((GROUPS, LIVE), 1).astype(F32)
    cap_row = g[:1] + jnp.sum(jnp.where(g >= end_col, CAP - count_col, 0.0), axis=0, keepdims=True)
    g = iota((LIVE, GROUPS), 0).astype(F32)
    more = jnp.where(g >= end_row, CAP - count_row[:1], 0.0)
    cap_col = g[:, :1] + jnp.sum(more, axis=1, keepdims=True)
    lanes = iota((LIVE, CAP), 1).astype(F32)
    for j in range(GROUPS):
        at = slice(j * CAP, (j + 1) * CAP)
        spread[at, :] = chosen(cap_row - float(j * CAP))
        packed[:, at] = (cap_col - float(j * CAP) == lanes).astype(BF16)


def cross_maps(pos):
    wide = GROUPS * CAP
    return call(
        cross_body,
        (jax.ShapeDtypeStruct((wide, LIVE), BF16), jax.ShapeDtypeStruct((LIVE, wide), BF16)),
        [VM],
        (VM, VM),
        "cross_maps",
        1 << 28,
        3 << 20,
        6,
    )(pos)


def chosen(pos_row, cap=CAP):
    shape = (cap, pos_row.shape[1])
    return (iota(shape, 0).astype(F32) == pos_row).astype(BF16)


def halves(squares):
    high = squares.astype(BF16)
    return high, (squares - high.astype(F32)).astype(BF16)


def project(x, layer, gain_ref, weights, outs, at):
    normed = (x * gain_ref[layer : layer + 1, :]).astype(BF16)
    width = weights[0].shape[2]
    for n, weight in enumerate(weights):
        found = mm(normed, weight[layer]).astype(BF16)
        for side, out in enumerate(outs):
            out[at, :CAP, n * width : (n + 1) * width] = found[side * CAP : (side + 1) * CAP]
    squares = x * x
    squares = sum(squares[:, n : n + CAP] for n in range(0, x.shape[1], CAP))
    ones = jnp.ones((8, CAP), BF16)
    high, low = halves(squares)
    squares = mm(ones, high, ((1,), (1,))) + mm(ones, low, ((1,), (1,)))
    for side, out in enumerate(outs):
        high, low = halves(squares[:, side * CAP : (side + 1) * CAP])
        out[at, CAP:, :] = jnp.zeros((8, out.shape[2]), BF16)
        out[at, CAP:, :CAP] = high
        out[at, CAP:, CAP : 2 * CAP] = low


def spread_rows(spread, j):
    return spread[pl.ds(pl.multiple_of(j * CAP, CAP), CAP), :]


def pair_at(i):
    core, _, _ = place_of()
    return 2 * i + core, 2 * i + 1 - core


def first_body(layer, x_ref, pos_ref, gain_ref, *refs):
    weights, (own_ref, sent_ref, x_out) = refs[:4], refs[4:]

    def step(i, _):
        rows = [mm(chosen(pos_ref[pl.ds(j, 1), :]), x_ref[j]) for j in pair_at(i)]
        for j, x in zip(pair_at(i), rows):
            x_out[j] = x.astype(BF16)
        project(jnp.concatenate(rows, 0), layer, gain_ref, weights, (own_ref, sent_ref), i)
        return 0

    lax.fori_loop(0, 4, step, 0)


def gathered(y, updates, update):
    part = updates[0].shape[0]
    for d, u in enumerate(updates):
        update[pl.ds(pl.multiple_of(((y + 4 - d) % 4) * part, part), part), :] = u[...]


def next_body(layer, x_ref, spread, u0, u1, u2, u3, gain_ref, *refs):
    weights, (own_ref, sent_ref, x_out, update) = refs[:4], refs[4:]
    _, _, p = place_of()
    gathered(p, (u0, u1, u2, u3), update)

    def step(i, _):
        picked = jnp.concatenate([spread_rows(spread, j) for j in pair_at(i)], 0)
        x = jnp.concatenate([x_ref[j] for j in pair_at(i)], 0)
        x = (x.astype(F32) + mm(picked, update[...])).astype(BF16)
        for side, j in enumerate(pair_at(i)):
            x_out[j] = x[side * CAP : (side + 1) * CAP]
        project(x.astype(F32), layer, gain_ref, weights, (own_ref, sent_ref), i)
        return 0

    lax.fori_loop(0, 4, step, 0)


def projections(layer, x, maps, updates, gain, weights):
    features = x.shape[-1]
    width = 4 * weights[0].shape[2]
    args = [x, maps, *updates, gain, *weights]
    return call(
        functools.partial(next_body if updates else first_body, layer),
        (
            jax.ShapeDtypeStruct((4, CAP + 8, width), BF16),
            jax.ShapeDtypeStruct((4, CAP + 8, width), BF16),
            jax.ShapeDtypeStruct((GROUPS, CAP, features), BF16),
        ),
        [VM] * len(args),
        (VM,) * 3,
        "next_projection" if updates else "first_projection",
        2 << 30,
        6 << 20,
        scratch_shapes=[pltpu.VMEM((LIVE, features), BF16)] if updates else [],
    )(*args)


def pair_body(own_ref, got_ref, keep_ref, *sent):
    _, x, _ = place_of()

    def step(d, keep):
        at = (x + d) % 4
        squares = own_ref[at, CAP:, : 2 * CAP].astype(F32) + got_ref[at, CAP:, : 2 * CAP].astype(F32)
        squares = squares[:, :CAP] + squares[:, CAP:]
        high = squares if keep else squares.astype(BF16)
        low = squares - high.astype(F32)
        out = keep_ref if keep else sent[d - 1]
        kind = out.dtype
        out[CAP:, :CAP] = high.astype(kind)
        out[CAP:, CAP : 2 * CAP] = low.astype(kind)
        for n in range(0, own_ref.shape[2], 256):
            piece = own_ref[at, :CAP, n : n + 256].astype(F32) + got_ref[at, :CAP, n : n + 256].astype(F32)
            out[:CAP, n : n + 256] = piece.astype(kind)
        out[CAP:, 2 * CAP :] = jnp.zeros((8, own_ref.shape[2] - 2 * CAP), kind)

    for d in (2, 1, 3, 0):
        step(d, d == 0)


def pair_sum(own, got):
    rows, width = own.shape[1:]
    return call(
        pair_body,
        (jax.ShapeDtypeStruct((rows, width), F32),)
        + (jax.ShapeDtypeStruct((rows, width), BF16),) * 3,
        [VM, VM],
        (VM,) * 4,
        "pair_sum",
        1 << 20,
        4 << 20,
        8,
    )(own, got)


def roll_slots(x, d):
    return pltpu.roll(x, d, 1) if d else x


def read_body(layer, keep, r1, r2, r3, pos_ref, low_ref, extra_ref, chan_ref, states, *refs):
    out_rows, kk, vv, wide, alive, more, past, qa, reads, gates = refs
    heads = kk.shape[0]
    seqs = kk.shape[1]
    rows = seqs * SLOTS
    dim = 128
    total = (keep[...] + r1[...].astype(F32)) + (r2[...].astype(F32) + r3[...].astype(F32))
    squares = total[CAP : CAP + 1, :CAP] + total[CAP : CAP + 1, CAP : 2 * CAP]
    scale = lax.rsqrt(squares / D + EPSILON)
    eye = iota((CAP, CAP), 0) == iota((CAP, CAP), 1)
    scale = jnp.sum(jnp.where(eye, scale, 0.0), axis=1, keepdims=True)
    scaled = (total[:CAP] * scale).astype(BF16)
    picked = chosen(pos_ref[pl.ds(lax.axis_index("dp"), 1), :])
    wide[...] = mm(picked, scaled, ((0,), (0,)))
    alive[...] = mm(picked, jnp.ones((CAP, dim), BF16), ((0,), (0,)))
    for h in range(heads):
        row = extra_ref[layer, h : h + 1, :]
        more[h] = jnp.transpose(jnp.broadcast_to(row, (dim, rows)))
    some = 8
    chunk = some * SLOTS
    shape = (some, SLOTS, dim)

    def prepare(n, _):
        h, c = n // (seqs // some), n % (seqs // some)
        at = pl.ds(pl.multiple_of(c * chunk, chunk), chunk)
        here = pl.ds(c * some, some)

        def part(k):
            lanes = pl.ds(pl.multiple_of((k * heads + h) * dim, dim), dim)
            return wide[at, lanes].reshape(shape)

        lanes = pl.ds(pl.multiple_of(h * dim, dim), dim)
        low = low_ref[layer : layer + 1, lanes]
        chan = chan_ref[layer : layer + 1, lanes]
        extra = more[h, at, :].reshape(shape)
        live = alive[at, :].reshape(shape) > 0.5
        slot = iota(shape, 1)
        query = jax.nn.silu(part(0))
        forget = part(1)
        left = low + (1.0 - low) * jax.nn.sigmoid(forget)
        key = jnp.where(live, (1.0 - low) * jax.nn.sigmoid(-forget), 0.0)
        value = part(2)
        decay = jnp.log(jnp.maximum(left, TINY)) + extra
        decay = jnp.where(live, decay, 0.0)
        for d in (1, 2, 4):
            decay = decay + jnp.where(slot >= d, roll_slots(decay, d), 0.0)
        ones = jnp.ones((dim, dim), BF16)
        read = jnp.zeros(shape, F32)
        for n, what in enumerate((key, decay, value)):
            past[n] = what
        for j in range(SLOTS):
            at_j = pl.ds(j, 1)
            fade = jnp.exp(jnp.minimum(decay - past[1, :, at_j, :], 0.0))
            term = jnp.where(slot >= j, query * past[0, :, at_j, :] * fade, 0.0)
            weight = mm(term.astype(BF16).reshape(chunk, dim), ones)
            read = read + weight.reshape(shape) * past[2, :, at_j, :]
        reads[h, here] = read
        qa[h, here] = (query * jnp.exp(decay)).astype(BF16)
        last = decay[:, SLOTS - 1 :, :]
        whole = jnp.exp(last)
        high = whole.astype(BF16).astype(F32)
        tail = jnp.where(slot == 0, high, jnp.where(slot == 1, whole - high, 0.0))
        kk[h, here, :SLOTS, :] = (key * jnp.exp(last - decay)).astype(BF16)
        kk[h, here, SLOTS:, :] = tail.astype(BF16)
        vv[h, here] = value.astype(BF16)
        gates[h, here] = jax.nn.silu(part(3)) * chan
        return 0

    lax.fori_loop(0, heads * (seqs // some), prepare, 0)

    def apply(n, _):
        for s in range(4):
            at = 4 * n + s
            for h in range(heads):
                reads[h, at] += mm(qa[h, at], states[layer, at, h].astype(BF16))
        return 0

    lax.fori_loop(0, seqs // 4, apply, 0)
    for h in range(heads):
        read = reads[h]
        mean = jnp.mean(read * read, axis=-1, keepdims=True)
        head = (read * lax.rsqrt(mean + EPSILON) * gates[h]).astype(BF16).reshape(rows, dim)
        out_rows[:, h * dim : (h + 1) * dim] = mm(picked, head).astype(BF16)


def read_states(layer, keep, got, pos, low, extra, chan, states):
    _, seqs, heads, dim, _ = states.shape
    return call(
        functools.partial(read_body, layer),
        (
            jax.ShapeDtypeStruct((CAP, heads * dim), BF16),
            jax.ShapeDtypeStruct((heads, seqs, 2 * SLOTS, dim), BF16),
            jax.ShapeDtypeStruct((heads, seqs, SLOTS, dim), BF16),
        ),
        [VM] * 9,
        (VM,) * 3,
        "read_states",
        1 << 30,
        6 << 20,
        12,
        scratch_shapes=[
            pltpu.VMEM((seqs * SLOTS, 4 * heads * dim), F32),
            pltpu.VMEM((seqs * SLOTS, dim), F32),
            pltpu.VMEM((heads, seqs * SLOTS, dim), F32),
            pltpu.VMEM((3, 8, SLOTS, dim), F32),
            pltpu.VMEM((heads, seqs, SLOTS, dim), BF16),
            pltpu.VMEM((heads, seqs, SLOTS, dim), F32),
            pltpu.VMEM((heads, seqs, SLOTS, dim), F32),
        ],
    )(keep, *got, pos, low, jnp.swapaxes(extra, 1, 2), chan, states)


def write_body(kk, vv, state_ref, *refs):
    out_state = refs[-1]
    dim = 128
    zero = jnp.zeros((SLOTS, dim), BF16)
    ones = jnp.ones((SLOTS, dim), BF16)

    def one(s, _):
        for h in range(state_ref.shape[2]):
            state = state_ref[0, s, h]
            values = jnp.concatenate(
                [jnp.concatenate([vv[h, s], zero], 1), jnp.concatenate([zero, ones], 1)], 0
            )
            both = mm(kk[h, s], values, ((0,), (0,)))
            out_state[0, s, h] = both[:, dim:] * state + both[:, :dim]
        return 0

    lax.fori_loop(0, state_ref.shape[1], one, 0)


def write_states(layer, half, kk, vv, states, written):
    _, seqs, heads, dim, _ = states.shape
    here = 4
    first = half * (seqs // here // 2)
    block = pl.BlockSpec((1, here, heads, dim, dim), lambda i: (layer, first + i, 0, 0, 0))
    small = lambda a: pl.BlockSpec((heads, here, a.shape[2], dim), lambda i: (0, first + i, 0, 0))
    more = [] if written is None else [written]
    return call(
        write_body,
        jax.ShapeDtypeStruct(states.shape, F32),
        [small(kk), small(vv), block] + [pl.BlockSpec(memory_space=pl.ANY)] * len(more),
        block,
        "write_states",
        5 << 30,
        4 << 20,
        8,
        grid=(seqs // here // 2,),
        input_output_aliases={3: 0} if more else {},
    )(kk, vv, states, *more)


def emit_body(layer, *refs):
    blocks, (packed, weight, keep_ref, s1, s2, s3, held, rows) = refs[:8], refs[8:]
    core, x, y = place_of()
    for side in range(2):
        for d in range(4):
            j = 2 * ((x + 4 - d) % 4) + (1 - core if side else core)
            held[pl.ds(pl.multiple_of(j * CAP, CAP), CAP), :] = blocks[4 * side + d][...]
    part = keep_ref.shape[0]
    rows[...] = mm(packed[...], held[...]).astype(BF16)
    for d in (2, 1, 3, 0):
        at = pl.multiple_of(((y + d) % 4) * part, part)
        out = mm(rows[pl.ds(at, part), :], weight[layer])
        if d == 0:
            keep_ref[...] = out
        else:
            (s1, s2, s3)[d - 1][...] = out.astype(BF16)


def emission(layer, blocks, packed, weight):
    width = weight.shape[2]
    part = LIVE // 4
    return call(
        functools.partial(emit_body, layer),
        (jax.ShapeDtypeStruct((part, width), F32),)
        + (jax.ShapeDtypeStruct((part, width), BF16),) * 3,
        [VM] * 10,
        (VM,) * 4,
        "emission",
        1 << 29,
        3 << 20,
        10,
        scratch_shapes=[pltpu.VMEM((n, blocks[0].shape[1]), BF16) for n in (GROUPS * CAP, LIVE)],
    )(*blocks, packed, weight)


def dead_body(x_in, pos_ref, out):
    place = chosen(pos_ref[pl.ds(pl.program_id(0), 1), :])
    live = mm(place, jnp.ones((CAP, 128), BF16), ((0,), (0,))) > 0.5
    for at in range(0, x_in.shape[2], 128):
        old = x_in[0, :, at : at + 128].astype(F32)
        out[0, :, at : at + 128] = jnp.where(live, 0.0, old).astype(BF16)


def dead_rows(x_in, pos):
    groups, slots, features = x_in.shape
    block = pl.BlockSpec((1, slots, features), lambda i: (i, 0, 0))
    return call(
        dead_body,
        jax.ShapeDtypeStruct(x_in.shape, BF16),
        [block, pl.BlockSpec(pos.shape, lambda i: (0, 0))],
        block,
        "dead_rows",
        1 << 28,
        4 << 20,
        6,
        grid=(groups,),
    )(x_in, pos)


def last_body(x_all, dead, pos_ref, spread, u0, u1, u2, u3, out, update, fresh_x, held, sems):
    _, _, p = place_of()
    gathered(p, (u0, u1, u2, u3), update)

    def apply(i, _):
        picked = jnp.concatenate([spread_rows(spread, j) for j in pair_at(i)], 0)
        x = jnp.concatenate([x_all[j] for j in pair_at(i)], 0)
        x = (x.astype(F32) + mm(picked, update[...])).astype(BF16)
        for side, j in enumerate(pair_at(i)):
            fresh_x[j] = x[side * CAP : (side + 1) * CAP]
        return 0

    lax.fori_loop(0, 4, apply, 0)

    def sending(j):
        return pltpu.make_async_copy(held.at[j], out.at[j], sems.at[j])

    def place(j, _):
        picked = chosen(pos_ref[pl.ds(j, 1), :])
        held[j] = mm(picked, fresh_x[j], ((0,), (0,))).astype(BF16) + dead[j]
        sending(j).start()
        return 0

    def finish(j, _):
        sending(j).wait()
        return 0

    lax.fori_loop(0, GROUPS, place, 0)
    lax.fori_loop(0, GROUPS, finish, 0)


def last_rows(x_all, dead, pos, spread, updates):
    groups, slots, features = dead.shape
    return call(
        last_body,
        pltpu.HBM(dead.shape, BF16),
        [VM] * 8,
        pl.BlockSpec(memory_space=pltpu.HBM),
        "last_rows",
        1 << 30,
        6 << 20,
        16,
        scratch_shapes=[
            pltpu.VMEM((LIVE, features), BF16),
            pltpu.VMEM((GROUPS, CAP, features), BF16),
            pltpu.VMEM(dead.shape, BF16),
            pltpu.SemaphoreType.DMA((GROUPS,)),
        ],
    )(x_all, dead, pos, spread, *updates)


def to_core(a):
    return lax.ppermute(a, "dp", [(i, i ^ 1) for i in range(8)])


def to_x(a, d):
    return lax.ppermute(a, "dp", [(i, (i + 2 * d) % 8) for i in range(8)])


def along(a, d, second):
    pairs = []
    for i in range(128):
        z, y, rest, core = i // 32, i // 8 % 4, i % 8, i % 2
        if core == second:
            y = (y + d) % 4
        else:
            z = (z + d) % 4
        pairs.append((i, z * 32 + y * 8 + rest))
    return lax.ppermute(a, ("tp", "dp"), pairs)


def fast(
    pos,
    activation_rows,
    entry_rescale_vector,
    probe_kernel,
    retention_kernel,
    content_kernel,
    valve_kernel,
    retention_minimum,
    extra_attenuation,
    channel_rescale_vector,
    emission_kernel,
    memory_grids,
):
    spread, packed = cross_maps(pos)
    rows, features = activation_rows.shape
    x_in = activation_rows.reshape(GROUPS, rows // GROUPS, features)
    weights = (probe_kernel, retention_kernel, content_kernel, valve_kernel)
    dead = dead_rows(x_in, pos)
    x, maps, updates, states = x_in, pos, (), None
    for layer in range(BLOCKS):
        own, sent, x = projections(layer, x, maps, updates, entry_rescale_vector, weights)
        keep, *sent = pair_sum(own, to_core(sent))
        got = [to_x(sent[d - 1], d) for d in (1, 2, 3)]
        if layer == 0:
            keep, spread, packed, dead = lax.optimization_barrier((keep, spread, packed, dead))
        yields, kk, vv = read_states(
            layer, keep, got, pos, retention_minimum, extra_attenuation,
            channel_rescale_vector, memory_grids,
        )
        states = write_states(layer, 0, kk, vv, memory_grids, states)
        mine = [yields] + [to_x(yields, d) for d in (1, 2, 3)]
        blocks = mine + [to_core(b) for b in mine]
        keep, *sent = emission(layer, blocks, packed, emission_kernel)
        a, b, c = [along(sent[d - 1], d, 0).astype(F32) for d in (1, 2, 3)]
        part = (((keep + a) + b) + c).astype(BF16)
        part, states = lax.optimization_barrier((part, states))
        states = write_states(layer, 1, kk, vv, memory_grids, states)
        a, b, c = [along(part, d, 1).astype(F32) for d in (1, 2, 3)]
        share = ((part.astype(F32) + b) + (a + c)).astype(BF16)
        share, states = lax.optimization_barrier((share, states))
        updates = [share] + [along(share, d, 0) for d in (1, 2, 3)]
        maps = spread
    mixed = last_rows(x, dead, pos, spread, updates)
    return mixed.reshape(rows, features), states


def exchanged(pieces, axis):
    return lax.all_to_all(pieces, axis, split_axis=0, concat_axis=0, tiled=True)


def collect(shard, axis):
    pieces = exchanged(jnp.broadcast_to(shard, (lax.axis_size(axis), *shard.shape)), axis)
    return pieces.reshape(-1, shard.shape[1])


def sum_at_owner(partial, axis):
    count = lax.axis_size(axis)
    pieces = partial.reshape(count, partial.shape[0] // count, partial.shape[1])
    return exchanged(pieces, axis).astype(F32).sum(axis=0)


def general_tick(scores, low, extra, chan, spans, states):
    seqs, heads, dim, _ = states.shape
    query, forget, value, gate = [
        jnp.moveaxis(s.astype(F32).reshape(seqs, SLOTS, heads, dim), 1, 0) for s in scores
    ]
    low = low.reshape(heads, dim)
    query = jax.nn.silu(query)
    decay = jnp.log(low + (1.0 - low) * jax.nn.sigmoid(forget))
    decay = decay + jnp.moveaxis(extra.reshape(seqs, SLOTS, heads), 1, 0)[..., None]
    key = (1.0 - low) * jax.nn.sigmoid(-forget)
    live = jnp.arange(SLOTS)[:, None] < spans[None, :]

    def advance(state, now):
        q, k, a, v, on = now
        fresh = jnp.exp(a)[..., None] * state + k[..., None] * v[..., None, :]
        state = jnp.where(on[:, None, None, None], fresh, state)
        return state, jnp.einsum("shkv,shk->shv", state, q)

    states, read = lax.scan(advance, states, (query, key, decay, value, live))
    read = read * lax.rsqrt(jnp.mean(read * read, axis=-1, keepdims=True) + EPSILON)
    read = read * chan.reshape(heads, dim) * jax.nn.silu(gate)
    read = jnp.where(live[:, :, None, None], read, 0.0)
    return jnp.moveaxis(read, 0, 1).reshape(seqs * SLOTS, heads * dim).astype(BF16), states


def general(
    fresh_spans,
    activation_rows,
    entry_rescale_vector,
    probe_kernel,
    retention_kernel,
    content_kernel,
    valve_kernel,
    retention_minimum,
    extra_attenuation,
    channel_rescale_vector,
    emission_kernel,
    memory_grids,
):
    groups = lax.axis_size("dp")
    rows = activation_rows.shape[0] // groups

    def block(current, layer):
        gain, q, f, v, g, low, extra, chan, out, states = layer
        squares = lax.psum(jnp.sum(current * current, axis=1), "dp")
        scale = lax.rsqrt(squares / D + EPSILON)
        normed = (current * gain).astype(BF16)
        partial = jnp.concatenate(
            [jnp.dot(normed, w, preferred_element_type=F32).astype(BF16) for w in (q, f, v, g)], axis=1
        )
        own = lax.dynamic_slice_in_dim(scale, lax.axis_index("dp") * rows, rows, 0)
        scaled = (sum_at_owner(partial, "dp") * own[:, None]).astype(BF16)
        yields, states = general_tick(
            jnp.split(scaled, 4, axis=1), low, extra, chan, fresh_spans, states
        )
        partial = jnp.dot(collect(yields, "dp"), out, preferred_element_type=F32).astype(BF16)
        update = collect(sum_at_owner(partial, "tp").astype(BF16), "tp")
        return (current + update.astype(F32)).astype(BF16).astype(F32), states

    mixed, states = lax.scan(
        block,
        activation_rows.astype(F32),
        (
            entry_rescale_vector,
            probe_kernel,
            retention_kernel,
            content_kernel,
            valve_kernel,
            retention_minimum,
            extra_attenuation,
            channel_rescale_vector,
            emission_kernel,
            memory_grids,
        ),
    )
    return mixed.astype(BF16), states


def local(activation_rows, fresh_spans, *rest):
    count = fresh_spans.shape[0]
    spans = lax.dynamic_update_slice(
        jnp.zeros((GROUPS * count,), jnp.int32), fresh_spans, (lax.axis_index("dp") * count,)
    )
    spans = lax.psum(spans, "dp")
    pos, fits = index_maps(spans)
    return lax.cond(
        fits[0] > 0,
        lambda: fast(pos, activation_rows, *rest),
        lambda: general(fresh_spans, activation_rows, *rest),
    )


def solution(mesh):
    placed = (
        P(None, "dp"),
        P("dp"),
        P(None, "dp"),
        P(None, "dp", "tp"),
        P(None, "dp", "tp"),
        P(None, "dp", "tp"),
        P(None, "dp", "tp"),
        P(None, "tp"),
        P(None, "dp", "tp"),
        P(None, "tp"),
        P(None, "tp", "dp"),
        P(None, "dp", "tp", None, None),
    )
    return jax.shard_map(
        local,
        mesh=mesh,
        in_specs=placed,
        out_specs=(P(None, "dp"), P(None, "dp", "tp", None, None)),
        check_vma=False,
    )
```

```python
import functools

import jax
import jax.numpy as jnp
from jax import lax
from jax.experimental import pallas as pl
from jax.experimental.pallas import tpu as pltpu
from jax.sharding import PartitionSpec as P

D = 4096
BLOCKS = 2
EPSILON = 1e-05
GROUPS = 8
CAP = 128
LIVE = 768
SLOTS = 8
TINY = 1.2e-38
F32 = jnp.float32
BF16 = jnp.bfloat16
VM = pl.BlockSpec(memory_space=pltpu.VMEM)


def iota(shape, dim):
    return lax.broadcasted_iota(jnp.int32, shape, dim)


def mm(a, b, dims=((1,), (0,)), **kw):
    return lax.dot_general(a, b, (dims, ((), ())), preferred_element_type=F32, **kw)


def call(body, out_shape, in_specs, out_specs, name, flops=0, moved=0, vmem=16, **kw):
    return pl.pallas_call(
        body,
        out_shape=out_shape,
        in_specs=in_specs,
        out_specs=out_specs,
        name=name,
        cost_estimate=pl.CostEstimate(flops=flops, bytes_accessed=moved, transcendentals=0),
        compiler_params=pltpu.CompilerParams(vmem_limit_bytes=vmem << 20),
        **kw,
    )


def place_of():
    tp, dp = lax.axis_index("tp"), lax.axis_index("dp")
    core = dp % 2
    return core, dp // 2, jnp.where(core == 0, tp % 4, tp // 4)


def index_body(spans_ref, pos_ref, fits_ref):
    total = spans_ref.shape[1]
    seqs = total // GROUPS
    rows = seqs * SLOTS
    row = spans_ref[...].astype(F32)
    spans = jnp.where(iota((GROUPS, total), 1) // seqs == iota((GROUPS, total), 0), row, 0.0)
    at, slot = iota((total, rows), 0) % seqs, iota((total, rows), 1) // SLOTS
    start = mm(spans, (at < slot).astype(F32))
    span = mm(spans, (at == slot).astype(F32))
    slot = (iota((GROUPS, rows), 1) % SLOTS).astype(F32)
    pos_ref[...] = jnp.where(slot < span, start + slot, -1.0)
    count_col = jnp.sum(spans, axis=1, keepdims=True)
    fits_ref[0] = (jnp.max(count_col) <= CAP).astype(jnp.int32)


def index_maps(spans):
    rows = spans.shape[0] // GROUPS * SLOTS
    return call(
        index_body,
        (
            jax.ShapeDtypeStruct((GROUPS, rows), F32),
            jax.ShapeDtypeStruct((1,), jnp.int32),
        ),
        [VM],
        (VM, pl.BlockSpec(memory_space=pltpu.SMEM)),
        "index_maps",
        1 << 20,
        1 << 20,
        4,
    )(spans.reshape(1, -1))


def cross_body(pos_ref, spread, packed):
    rows = pos_ref.shape[1]
    live = (pos_ref[...] >= 0.0).astype(F32)
    count_col = jnp.sum(live, axis=1, keepdims=True)
    count_row = mm(jnp.ones((GROUPS, rows), F32), live, ((1,), (1,)))
    upto = (iota((GROUPS, GROUPS), 1) <= iota((GROUPS, GROUPS), 0)).astype(F32)
    end_col = mm(upto, jnp.broadcast_to(count_col, (GROUPS, 128)))[:, :1]
    end_row = mm(count_row, upto, ((1,), (1,)))[:1]
    g = iota((GROUPS, LIVE), 1).astype(F32)
    cap_row = g[:1] + jnp.sum(jnp.where(g >= end_col, CAP - count_col, 0.0), axis=0, keepdims=True)
    g = iota((LIVE, GROUPS), 0).astype(F32)
    more = jnp.where(g >= end_row, CAP - count_row[:1], 0.0)
    cap_col = g[:, :1] + jnp.sum(more, axis=1, keepdims=True)
    lanes = iota((LIVE, CAP), 1).astype(F32)
    for j in range(GROUPS):
        at = slice(j * CAP, (j + 1) * CAP)
        spread[at, :] = chosen(cap_row - float(j * CAP))
        packed[:, at] = (cap_col - float(j * CAP) == lanes).astype(BF16)


def cross_maps(pos):
    wide = GROUPS * CAP
    return call(
        cross_body,
        (jax.ShapeDtypeStruct((wide, LIVE), BF16), jax.ShapeDtypeStruct((LIVE, wide), BF16)),
        [VM],
        (VM, VM),
        "cross_maps",
        1 << 28,
        3 << 20,
        6,
    )(pos)


def chosen(pos_row, cap=CAP):
    shape = (cap, pos_row.shape[1])
    return (iota(shape, 0).astype(F32) == pos_row).astype(BF16)


def halves(squares):
    high = squares.astype(BF16)
    return high, (squares - high.astype(F32)).astype(BF16)


def project(x, layer, gain_ref, weights, outs, at):
    normed = (x * gain_ref[layer : layer + 1, :]).astype(BF16)
    width = weights[0].shape[2]
    for n, weight in enumerate(weights):
        found = mm(normed, weight[layer]).astype(BF16)
        for side, out in enumerate(outs):
            out[at, :CAP, n * width : (n + 1) * width] = found[side * CAP : (side + 1) * CAP]
    squares = x * x
    squares = sum(squares[:, n : n + CAP] for n in range(0, x.shape[1], CAP))
    ones = jnp.ones((8, CAP), BF16)
    high, low = halves(squares)
    squares = mm(ones, high, ((1,), (1,))) + mm(ones, low, ((1,), (1,)))
    for side, out in enumerate(outs):
        high, low = halves(squares[:, side * CAP : (side + 1) * CAP])
        out[at, CAP:, :] = jnp.zeros((8, out.shape[2]), BF16)
        out[at, CAP:, :CAP] = high
        out[at, CAP:, CAP : 2 * CAP] = low


def spread_rows(spread, j):
    return spread[pl.ds(pl.multiple_of(j * CAP, CAP), CAP), :]


def pair_at(i):
    core, _, _ = place_of()
    return 2 * i + core, 2 * i + 1 - core


def first_body(layer, x_ref, pos_ref, gain_ref, *refs):
    weights, (own_ref, sent_ref, x_out) = refs[:4], refs[4:]

    def step(i, _):
        rows = [mm(chosen(pos_ref[pl.ds(j, 1), :]), x_ref[j]) for j in pair_at(i)]
        for j, x in zip(pair_at(i), rows):
            x_out[j] = x.astype(BF16)
        project(jnp.concatenate(rows, 0), layer, gain_ref, weights, (own_ref, sent_ref), i)
        return 0

    lax.fori_loop(0, 4, step, 0)


def gathered(y, updates, update):
    part = updates[0].shape[0]
    for d, u in enumerate(updates):
        update[pl.ds(pl.multiple_of(((y + 4 - d) % 4) * part, part), part), :] = u[...]


def next_body(layer, x_ref, spread, u0, u1, u2, u3, gain_ref, *refs):
    weights, (own_ref, sent_ref, x_out, update) = refs[:4], refs[4:]
    _, _, p = place_of()
    gathered(p, (u0, u1, u2, u3), update)

    def step(i, _):
        picked = jnp.concatenate([spread_rows(spread, j) for j in pair_at(i)], 0)
        x = jnp.concatenate([x_ref[j] for j in pair_at(i)], 0)
        x = (x.astype(F32) + mm(picked, update[...])).astype(BF16)
        for side, j in enumerate(pair_at(i)):
            x_out[j] = x[side * CAP : (side + 1) * CAP]
        project(x.astype(F32), layer, gain_ref, weights, (own_ref, sent_ref), i)
        return 0

    lax.fori_loop(0, 4, step, 0)


def projections(layer, x, maps, updates, gain, weights):
    features = x.shape[-1]
    width = 4 * weights[0].shape[2]
    args = [x, maps, *updates, gain, *weights]
    return call(
        functools.partial(next_body if updates else first_body, layer),
        (
            jax.ShapeDtypeStruct((4, CAP + 8, width), BF16),
            jax.ShapeDtypeStruct((4, CAP + 8, width), BF16),
            jax.ShapeDtypeStruct((GROUPS, CAP, features), BF16),
        ),
        [VM] * len(args),
        (VM,) * 3,
        "next_projection" if updates else "first_projection",
        2 << 30,
        6 << 20,
        scratch_shapes=[pltpu.VMEM((LIVE, features), BF16)] if updates else [],
    )(*args)


def pair_body(own_ref, got_ref, keep_ref, *sent):
    _, x, _ = place_of()

    def step(d, keep):
        at = (x + d) % 4
        squares = own_ref[at, CAP:, : 2 * CAP].astype(F32) + got_ref[at, CAP:, : 2 * CAP].astype(F32)
        squares = squares[:, :CAP] + squares[:, CAP:]
        high = squares if keep else squares.astype(BF16)
        low = squares - high.astype(F32)
        out = keep_ref if keep else sent[d - 1]
        kind = out.dtype
        out[CAP:, :CAP] = high.astype(kind)
        out[CAP:, CAP : 2 * CAP] = low.astype(kind)
        for n in range(0, own_ref.shape[2], 256):
            piece = own_ref[at, :CAP, n : n + 256].astype(F32) + got_ref[at, :CAP, n : n + 256].astype(F32)
            out[:CAP, n : n + 256] = piece.astype(kind)
        out[CAP:, 2 * CAP :] = jnp.zeros((8, own_ref.shape[2] - 2 * CAP), kind)

    for d in (2, 1, 3, 0):
        step(d, d == 0)


def pair_sum(own, got):
    rows, width = own.shape[1:]
    return call(
        pair_body,
        (jax.ShapeDtypeStruct((rows, width), F32),)
        + (jax.ShapeDtypeStruct((rows, width), BF16),) * 3,
        [VM, VM],
        (VM,) * 4,
        "pair_sum",
        1 << 20,
        4 << 20,
        8,
    )(own, got)


def roll_slots(x, d):
    return pltpu.roll(x, d, 1) if d else x


def read_body(layer, keep, r1, r2, r3, pos_ref, low_ref, extra_ref, chan_ref, states, *refs):
    out_rows, kk, vv, wide, alive, more, past, qa, reads, gates = refs
    heads = kk.shape[0]
    seqs = kk.shape[1]
    rows = seqs * SLOTS
    dim = 128
    total = (keep[...] + r1[...].astype(F32)) + (r2[...].astype(F32) + r3[...].astype(F32))
    squares = total[CAP : CAP + 1, :CAP] + total[CAP : CAP + 1, CAP : 2 * CAP]
    scale = lax.rsqrt(squares / D + EPSILON)
    eye = iota((CAP, CAP), 0) == iota((CAP, CAP), 1)
    scale = jnp.sum(jnp.where(eye, scale, 0.0), axis=1, keepdims=True)
    scaled = (total[:CAP] * scale).astype(BF16)
    picked = chosen(pos_ref[pl.ds(lax.axis_index("dp"), 1), :])
    wide[...] = mm(picked, scaled, ((0,), (0,)))
    alive[...] = mm(picked, jnp.ones((CAP, dim), BF16), ((0,), (0,)))
    for h in range(heads):
        row = extra_ref[layer, h : h + 1, :]
        more[h] = jnp.transpose(jnp.broadcast_to(row, (dim, rows)))
    some = 16
    chunk = some * SLOTS
    shape = (some, SLOTS, dim)

    def prepare(n, _):
        h, c = n // (seqs // some), n % (seqs // some)
        at = pl.ds(pl.multiple_of(c * chunk, chunk), chunk)
        here = pl.ds(c * some, some)

        def part(k):
            lanes = pl.ds(pl.multiple_of((k * heads + h) * dim, dim), dim)
            return wide[at, lanes].reshape(shape)

        lanes = pl.ds(pl.multiple_of(h * dim, dim), dim)
        low = low_ref[layer : layer + 1, lanes]
        chan = chan_ref[layer : layer + 1, lanes]
        extra = more[h, at, :].reshape(shape)
        live = alive[at, :].reshape(shape) > 0.5
        slot = iota(shape, 1)
        query = jax.nn.silu(part(0))
        forget = part(1)
        left = low + (1.0 - low) * jax.nn.sigmoid(forget)
        key = jnp.where(live, (1.0 - low) * jax.nn.sigmoid(-forget), 0.0)
        value = part(2)
        decay = jnp.log(jnp.maximum(left, TINY)) + extra
        decay = jnp.where(live, decay, 0.0)
        for d in (1, 2, 4):
            decay = decay + jnp.where(slot >= d, roll_slots(decay, d), 0.0)
        ones = jnp.ones((dim, dim), BF16)
        read = jnp.zeros(shape, F32)
        for n, what in enumerate((key, decay, value)):
            past[n] = what
        for j in range(SLOTS):
            at_j = pl.ds(j, 1)
            fade = jnp.exp(jnp.minimum(decay - past[1, :, at_j, :], 0.0))
            term = jnp.where(slot >= j, query * past[0, :, at_j, :] * fade, 0.0)
            weight = mm(term.astype(BF16).reshape(chunk, dim), ones)
            read = read + weight.reshape(shape) * past[2, :, at_j, :]
        reads[h, here] = read
        qa[h, here] = (query * jnp.exp(decay)).astype(BF16)
        last = decay[:, SLOTS - 1 :, :]
        whole = jnp.exp(last)
        high = whole.astype(BF16).astype(F32)
        tail = jnp.where(slot == 0, high, jnp.where(slot == 1, whole - high, 0.0))
        kk[h, here, :SLOTS, :] = (key * jnp.exp(last - decay)).astype(BF16)
        kk[h, here, SLOTS:, :] = tail.astype(BF16)
        vv[h, here] = value.astype(BF16)
        gates[h, here] = jax.nn.silu(part(3)) * chan
        return 0

    lax.fori_loop(0, heads * (seqs // some), prepare, 0)

    def apply(n, _):
        for s in range(4):
            at = 4 * n + s
            for h in range(heads):
                reads[h, at] += mm(qa[h, at], states[layer, at, h].astype(BF16))
        return 0

    lax.fori_loop(0, seqs // 4, apply, 0)
    for h in range(heads):
        read = reads[h]
        mean = jnp.mean(read * read, axis=-1, keepdims=True)
        head = (read * lax.rsqrt(mean + EPSILON) * gates[h]).astype(BF16).reshape(rows, dim)
        out_rows[:, h * dim : (h + 1) * dim] = mm(picked, head).astype(BF16)


def read_states(layer, keep, got, pos, low, extra, chan, states):
    _, seqs, heads, dim, _ = states.shape
    return call(
        functools.partial(read_body, layer),
        (
            jax.ShapeDtypeStruct((CAP, heads * dim), BF16),
            jax.ShapeDtypeStruct((heads, seqs, 2 * SLOTS, dim), BF16),
            jax.ShapeDtypeStruct((heads, seqs, SLOTS, dim), BF16),
        ),
        [VM] * 9,
        (VM,) * 3,
        "read_states",
        1 << 30,
        6 << 20,
        12,
        scratch_shapes=[
            pltpu.VMEM((seqs * SLOTS, 4 * heads * dim), F32),
            pltpu.VMEM((seqs * SLOTS, dim), F32),
            pltpu.VMEM((heads, seqs * SLOTS, dim), F32),
            pltpu.VMEM((3, 16, SLOTS, dim), F32),
            pltpu.VMEM((heads, seqs, SLOTS, dim), BF16),
            pltpu.VMEM((heads, seqs, SLOTS, dim), F32),
            pltpu.VMEM((heads, seqs, SLOTS, dim), F32),
        ],
    )(keep, *got, pos, low, jnp.swapaxes(extra, 1, 2), chan, states)


def write_body(kk, vv, state_ref, *refs):
    out_state = refs[-1]
    dim = 128
    zero = jnp.zeros((SLOTS, dim), BF16)
    ones = jnp.ones((SLOTS, dim), BF16)

    def one(s, _):
        for h in range(state_ref.shape[2]):
            state = state_ref[0, s, h]
            values = jnp.concatenate(
                [jnp.concatenate([vv[h, s], zero], 1), jnp.concatenate([zero, ones], 1)], 0
            )
            both = mm(kk[h, s], values, ((0,), (0,)))
            out_state[0, s, h] = both[:, dim:] * state + both[:, :dim]
        return 0

    lax.fori_loop(0, state_ref.shape[1], one, 0)


def write_states(layer, half, kk, vv, states, written):
    _, seqs, heads, dim, _ = states.shape
    here = 4
    first = half * (seqs // here // 2)
    block = pl.BlockSpec((1, here, heads, dim, dim), lambda i: (layer, first + i, 0, 0, 0))
    small = lambda a: pl.BlockSpec((heads, here, a.shape[2], dim), lambda i: (0, first + i, 0, 0))
    more = [] if written is None else [written]
    return call(
        write_body,
        jax.ShapeDtypeStruct(states.shape, F32),
        [small(kk), small(vv), block] + [pl.BlockSpec(memory_space=pl.ANY)] * len(more),
        block,
        "write_states",
        5 << 30,
        4 << 20,
        8,
        grid=(seqs // here // 2,),
        input_output_aliases={3: 0} if more else {},
    )(kk, vv, states, *more)


def emit_body(layer, *refs):
    blocks, (packed, weight, keep_ref, s1, s2, s3, held, rows) = refs[:8], refs[8:]
    core, x, y = place_of()
    for side in range(2):
        for d in range(4):
            j = 2 * ((x + 4 - d) % 4) + (1 - core if side else core)
            held[pl.ds(pl.multiple_of(j * CAP, CAP), CAP), :] = blocks[4 * side + d][...]
    part = keep_ref.shape[0]
    rows[...] = mm(packed[...], held[...]).astype(BF16)
    for d in (2, 1, 3, 0):
        at = pl.multiple_of(((y + d) % 4) * part, part)
        out = mm(rows[pl.ds(at, part), :], weight[layer])
        if d == 0:
            keep_ref[...] = out
        else:
            (s1, s2, s3)[d - 1][...] = out.astype(BF16)


def emission(layer, blocks, packed, weight):
    width = weight.shape[2]
    part = LIVE // 4
    return call(
        functools.partial(emit_body, layer),
        (jax.ShapeDtypeStruct((part, width), F32),)
        + (jax.ShapeDtypeStruct((part, width), BF16),) * 3,
        [VM] * 10,
        (VM,) * 4,
        "emission",
        1 << 29,
        3 << 20,
        10,
        scratch_shapes=[pltpu.VMEM((n, blocks[0].shape[1]), BF16) for n in (GROUPS * CAP, LIVE)],
    )(*blocks, packed, weight)


def dead_body(x_in, pos_ref, out):
    place = chosen(pos_ref[pl.ds(pl.program_id(0), 1), :])
    live = mm(place, jnp.ones((CAP, 128), BF16), ((0,), (0,))) > 0.5
    for at in range(0, x_in.shape[2], 128):
        old = x_in[0, :, at : at + 128].astype(F32)
        out[0, :, at : at + 128] = jnp.where(live, 0.0, old).astype(BF16)


def dead_rows(x_in, pos):
    groups, slots, features = x_in.shape
    block = pl.BlockSpec((1, slots, features), lambda i: (i, 0, 0))
    return call(
        dead_body,
        jax.ShapeDtypeStruct(x_in.shape, BF16),
        [block, pl.BlockSpec(pos.shape, lambda i: (0, 0))],
        block,
        "dead_rows",
        1 << 28,
        4 << 20,
        6,
        grid=(groups,),
    )(x_in, pos)


def last_body(x_all, dead, pos_ref, spread, u0, u1, u2, u3, out, update, fresh_x, held, sems):
    _, _, p = place_of()
    gathered(p, (u0, u1, u2, u3), update)

    def apply(i, _):
        picked = jnp.concatenate([spread_rows(spread, j) for j in pair_at(i)], 0)
        x = jnp.concatenate([x_all[j] for j in pair_at(i)], 0)
        x = (x.astype(F32) + mm(picked, update[...])).astype(BF16)
        for side, j in enumerate(pair_at(i)):
            fresh_x[j] = x[side * CAP : (side + 1) * CAP]
        return 0

    lax.fori_loop(0, 4, apply, 0)

    def sending(j):
        return pltpu.make_async_copy(held.at[j], out.at[j], sems.at[j])

    def place(j, _):
        picked = chosen(pos_ref[pl.ds(j, 1), :])
        held[j] = mm(picked, fresh_x[j], ((0,), (0,))).astype(BF16) + dead[j]
        sending(j).start()
        return 0

    def finish(j, _):
        sending(j).wait()
        return 0

    lax.fori_loop(0, GROUPS, place, 0)
    lax.fori_loop(0, GROUPS, finish, 0)


def last_rows(x_all, dead, pos, spread, updates):
    groups, slots, features = dead.shape
    return call(
        last_body,
        pltpu.HBM(dead.shape, BF16),
        [VM] * 8,
        pl.BlockSpec(memory_space=pltpu.HBM),
        "last_rows",
        1 << 30,
        6 << 20,
        16,
        scratch_shapes=[
            pltpu.VMEM((LIVE, features), BF16),
            pltpu.VMEM((GROUPS, CAP, features), BF16),
            pltpu.VMEM(dead.shape, BF16),
            pltpu.SemaphoreType.DMA((GROUPS,)),
        ],
    )(x_all, dead, pos, spread, *updates)


def to_core(a):
    return lax.ppermute(a, "dp", [(i, i ^ 1) for i in range(8)])


def to_x(a, d):
    return lax.ppermute(a, "dp", [(i, (i + 2 * d) % 8) for i in range(8)])


def along(a, d, second):
    pairs = []
    for i in range(128):
        z, y, rest, core = i // 32, i // 8 % 4, i % 8, i % 2
        if core == second:
            y = (y + d) % 4
        else:
            z = (z + d) % 4
        pairs.append((i, z * 32 + y * 8 + rest))
    return lax.ppermute(a, ("tp", "dp"), pairs)


def fast(
    pos,
    activation_rows,
    entry_rescale_vector,
    probe_kernel,
    retention_kernel,
    content_kernel,
    valve_kernel,
    retention_minimum,
    extra_attenuation,
    channel_rescale_vector,
    emission_kernel,
    memory_grids,
):
    spread, packed = cross_maps(pos)
    rows, features = activation_rows.shape
    x_in = activation_rows.reshape(GROUPS, rows // GROUPS, features)
    weights = (probe_kernel, retention_kernel, content_kernel, valve_kernel)
    dead = dead_rows(x_in, pos)
    x, maps, updates, states = x_in, pos, (), None
    for layer in range(BLOCKS):
        own, sent, x = projections(layer, x, maps, updates, entry_rescale_vector, weights)
        keep, *sent = pair_sum(own, to_core(sent))
        got = [to_x(sent[d - 1], d) for d in (1, 2, 3)]
        if layer == 0:
            keep, spread, packed, dead = lax.optimization_barrier((keep, spread, packed, dead))
        yields, kk, vv = read_states(
            layer, keep, got, pos, retention_minimum, extra_attenuation,
            channel_rescale_vector, memory_grids,
        )
        states = write_states(layer, 0, kk, vv, memory_grids, states)
        mine = [yields] + [to_x(yields, d) for d in (1, 2, 3)]
        blocks = mine + [to_core(b) for b in mine]
        keep, *sent = emission(layer, blocks, packed, emission_kernel)
        a, b, c = [along(sent[d - 1], d, 0).astype(F32) for d in (1, 2, 3)]
        part = (((keep + a) + b) + c).astype(BF16)
        part, states = lax.optimization_barrier((part, states))
        states = write_states(layer, 1, kk, vv, memory_grids, states)
        a, b, c = [along(part, d, 1).astype(F32) for d in (1, 2, 3)]
        share = ((part.astype(F32) + b) + (a + c)).astype(BF16)
        share, states = lax.optimization_barrier((share, states))
        updates = [share] + [along(share, d, 0) for d in (1, 2, 3)]
        maps = spread
    mixed = last_rows(x, dead, pos, spread, updates)
    return mixed.reshape(rows, features), states


def exchanged(pieces, axis):
    return lax.all_to_all(pieces, axis, split_axis=0, concat_axis=0, tiled=True)


def collect(shard, axis):
    pieces = exchanged(jnp.broadcast_to(shard, (lax.axis_size(axis), *shard.shape)), axis)
    return pieces.reshape(-1, shard.shape[1])


def sum_at_owner(partial, axis):
    count = lax.axis_size(axis)
    pieces = partial.reshape(count, partial.shape[0] // count, partial.shape[1])
    return exchanged(pieces, axis).astype(F32).sum(axis=0)


def general_tick(scores, low, extra, chan, spans, states):
    seqs, heads, dim, _ = states.shape
    query, forget, value, gate = [
        jnp.moveaxis(s.astype(F32).reshape(seqs, SLOTS, heads, dim), 1, 0) for s in scores
    ]
    low = low.reshape(heads, dim)
    query = jax.nn.silu(query)
    decay = jnp.log(low + (1.0 - low) * jax.nn.sigmoid(forget))
    decay = decay + jnp.moveaxis(extra.reshape(seqs, SLOTS, heads), 1, 0)[..., None]
    key = (1.0 - low) * jax.nn.sigmoid(-forget)
    live = jnp.arange(SLOTS)[:, None] < spans[None, :]

    def advance(state, now):
        q, k, a, v, on = now
        fresh = jnp.exp(a)[..., None] * state + k[..., None] * v[..., None, :]
        state = jnp.where(on[:, None, None, None], fresh, state)
        return state, jnp.einsum("shkv,shk->shv", state, q)

    states, read = lax.scan(advance, states, (query, key, decay, value, live))
    read = read * lax.rsqrt(jnp.mean(read * read, axis=-1, keepdims=True) + EPSILON)
    read = read * chan.reshape(heads, dim) * jax.nn.silu(gate)
    read = jnp.where(live[:, :, None, None], read, 0.0)
    return jnp.moveaxis(read, 0, 1).reshape(seqs * SLOTS, heads * dim).astype(BF16), states


def general(
    fresh_spans,
    activation_rows,
    entry_rescale_vector,
    probe_kernel,
    retention_kernel,
    content_kernel,
    valve_kernel,
    retention_minimum,
    extra_attenuation,
    channel_rescale_vector,
    emission_kernel,
    memory_grids,
):
    groups = lax.axis_size("dp")
    rows = activation_rows.shape[0] // groups

    def block(current, layer):
        gain, q, f, v, g, low, extra, chan, out, states = layer
        squares = lax.psum(jnp.sum(current * current, axis=1), "dp")
        scale = lax.rsqrt(squares / D + EPSILON)
        normed = (current * gain).astype(BF16)
        partial = jnp.concatenate(
            [jnp.dot(normed, w, preferred_element_type=F32).astype(BF16) for w in (q, f, v, g)], axis=1
        )
        own = lax.dynamic_slice_in_dim(scale, lax.axis_index("dp") * rows, rows, 0)
        scaled = (sum_at_owner(partial, "dp") * own[:, None]).astype(BF16)
        yields, states = general_tick(
            jnp.split(scaled, 4, axis=1), low, extra, chan, fresh_spans, states
        )
        partial = jnp.dot(collect(yields, "dp"), out, preferred_element_type=F32).astype(BF16)
        update = collect(sum_at_owner(partial, "tp").astype(BF16), "tp")
        return (current + update.astype(F32)).astype(BF16).astype(F32), states

    mixed, states = lax.scan(
        block,
        activation_rows.astype(F32),
        (
            entry_rescale_vector,
            probe_kernel,
            retention_kernel,
            content_kernel,
            valve_kernel,
            retention_minimum,
            extra_attenuation,
            channel_rescale_vector,
            emission_kernel,
            memory_grids,
        ),
    )
    return mixed.astype(BF16), states


def local(activation_rows, fresh_spans, *rest):
    count = fresh_spans.shape[0]
    spans = lax.dynamic_update_slice(
        jnp.zeros((GROUPS * count,), jnp.int32), fresh_spans, (lax.axis_index("dp") * count,)
    )
    spans = lax.psum(spans, "dp")
    pos, fits = index_maps(spans)
    return lax.cond(
        fits[0] > 0,
        lambda: fast(pos, activation_rows, *rest),
        lambda: general(fresh_spans, activation_rows, *rest),
    )


def solution(mesh):
    placed = (
        P(None, "dp"),
        P("dp"),
        P(None, "dp"),
        P(None, "dp", "tp"),
        P(None, "dp", "tp"),
        P(None, "dp", "tp"),
        P(None, "dp", "tp"),
        P(None, "tp"),
        P(None, "dp", "tp"),
        P(None, "tp"),
        P(None, "tp", "dp"),
        P(None, "dp", "tp", None, None),
    )
    return jax.shard_map(
        local,
        mesh=mesh,
        in_specs=placed,
        out_specs=(P(None, "dp"), P(None, "dp", "tp", None, None)),
        check_vma=False,
    )
```
